256 devices in a mesh: grp: 2 (over y), sp: 16 (over z), tp: 8 (over x, core).
Axes of the slice: x: 4, y: 2, z: 16, core: 2. Of those that a mesh axis runs over, the one named last changes fastest.
The devices are a block of a 4x16x16 slice.
Arguments:
- latent: bfloat16 [12288, 4096], P(('grp', 'sp')), parts along dimension 0, may hold values from -6 to 6
- context: bfloat16 [512, 4096], P(('grp', 'sp')), parts along dimension 0, may hold values from -6 to 6
- cond_latent: bfloat16 [8192], P('grp'), parts along dimension 0, may hold values from -6 to 6
- cond_context: bfloat16 [4096], replicated, may hold values from -6 to 6
- w_shift: bfloat16 [4096, 4096], P('sp', 'tp'), may hold values from -0.09375 to 0.09375
- w_scale: bfloat16 [4096, 4096], P('sp', 'tp'), may hold values from -0.09375 to 0.09375
- w_gate: bfloat16 [4096, 4096], P('sp', 'tp'), may hold values from -0.1875 to 0.1875
- norm_gain: float32 [4096], replicated, may hold values from 0.1 to 1.9
- w_query: bfloat16 [4096, 2048], P(None, 'tp'), may hold values from -0.09375 to 0.09375
- w_key: bfloat16 [4096, 1024], P(None, 'tp'), may hold values from -0.09375 to 0.09375
- w_value: bfloat16 [4096, 1024], P(None, 'tp'), may hold values from -0.09375 to 0.09375
- q_gain: float32 [128], replicated, may hold values from 1 to 6.5, as said below
- k_gain: float32 [128], replicated, may hold values from 1 to 6.5, as said below
- w_out: bfloat16 [2048, 4096], P('tp'), may hold values from -0.5 to 0.5
Outputs:
- mixed: bfloat16 [12288, 4096], P(('grp', 'sp', 'tp')), parts along dimension 0
The draws below stay inside these ranges and needn't reach their ends.
There are 2 independent parts, one for each index of `grp`. The reference program is written for one: setup_inputs(seed, part) draws one part's arguments, and reference() takes and returns one part's arrays. A program takes and returns all parts, laid end to end along the dimension named above; an argument that names none is the same for every part. Nothing has to cross between parts.
Inputs may be any that keep to these rules, and one draw needn't show every extreme that they name: `q_gain`: positive gains. `k_gain`: positive gains.
All inputs are finite; a program needn't handle non-finite values.
Results may differ from the reference program's by a relative error of at most 0.015.
The reference program's roundings to bfloat16 on the way (of `cond_act`, `normed`, `ctx_normed`, `queries`, `weights` and `attended`) count: a program that leaves them out, or rounds other values in their place, can miss the bound.
Values may be sent and summed in bfloat16 or wider, within the bound.
No kernel may reach another device: no remote copies, remote signals or barrier semaphores. Data moves between devices by JAX's collectives and lax.ppermute only.
A program may use at most 128 MiB of HBM per device.

```python
import math
import jax
import jax.numpy as jnp
from jax import lax

D = 4096
HEADS = 16
KV_HEADS = 8
HEAD = 128
GRID_W = 64
TOK_DEV = 384
CTX = 256
TOKENS = 6144
N_TP = 8


def gain_draw(key):
    return jnp.exp(jax.random.uniform(key, (HEAD,), jnp.float32, 0.0, math.log(2.5)))


def draw_q_gain(key, part):
    return gain_draw(jax.random.fold_in(key, 11))


def draw_k_gain(key, part):
    return gain_draw(jax.random.fold_in(key, 23))


def level_of(own_key, shape, cuts, least, high):
    def one(position, shards_of):
        steps = jax.random.uniform(jax.random.fold_in(jax.random.fold_in(own_key, 6), position), (shards_of,), jnp.float32, least / len(cuts), high / len(cuts))
        return jnp.repeat(jnp.exp(steps), shape[position] // shards_of).reshape((-1,) + (1,) * (len(shape) - position - 1))

    factor_of = one(*cuts[0])
    for cut in cuts[1:]:
        factor_of = factor_of * one(*cut)
    return factor_of


def noise(rng, shape, deviation, bound, cuts=(), kind=jnp.bfloat16):
    level = level_of(rng, shape, cuts, -0.22, 0.18) if cuts else 1.0
    drawn = jax.random.normal(rng, shape, jnp.float32) * deviation * level
    return jnp.minimum(jnp.maximum(drawn, -bound), bound).astype(kind)


def setup_inputs(seed: int = 0, part: int = 0) -> dict:
    seeds = jax.random.split(jax.random.key(seed), 15)
    part_keys = jax.random.split(jax.random.fold_in(seeds[14], part), 15)
    latent = noise(part_keys[0], (TOKENS, D), 1.0, 6.0, ((0, 16),))
    context = noise(part_keys[1], (CTX, D), 1.0, 6.0, ((0, 16),))
    cond_latent = noise(part_keys[2], (D,), 1.0, 6.0)
    cond_context = noise(seeds[3], (D,), 1.0, 6.0)
    w_shift = noise(seeds[4], (D, D), D ** -0.5, 0.09375, ((0, 16), (1, 8)))
    w_scale = noise(seeds[5], (D, D), D ** -0.5, 0.09375, ((0, 16), (1, 8)))
    w_gate = noise(seeds[6], (D, D), (D // 4) ** -0.5, 0.1875, ((0, 16), (1, 8)))
    norm_gain = jnp.clip(1.0 + 0.18 * jax.random.normal(seeds[7], (D,), jnp.float32), 0.1, 1.9)
    w_query = noise(seeds[8], (D, HEADS * HEAD), D ** -0.5, 0.09375, ((1, 8),))
    w_key = noise(seeds[9], (D, KV_HEADS * HEAD), D ** -0.5, 0.09375, ((1, 8),))
    w_value = noise(seeds[10], (D, KV_HEADS * HEAD), D ** -0.5, 0.09375, ((1, 8),))
    q_gain = draw_q_gain(jax.random.fold_in(seeds[14], 71), part)
    k_gain = draw_k_gain(jax.random.fold_in(seeds[14], 71), part)
    w_out = noise(seeds[13], (HEADS * HEAD, D), HEAD ** -0.5, 0.5, ((0, 8),))
    return dict(latent=latent, context=context, cond_latent=cond_latent, cond_context=cond_context, w_shift=w_shift, w_scale=w_scale, w_gate=w_gate, norm_gain=norm_gain, w_query=w_query, w_key=w_key, w_value=w_value, q_gain=q_gain, k_gain=k_gain, w_out=w_out)


epsilon = 1e-06
context_lift = 1.5
rope_theta = 10000.0

def rms_rows(values, gain):
    values = values.astype(jnp.float32)
    return values * lax.rsqrt(lax.optimization_barrier(jnp.mean(values * values, axis=-1, keepdims=True)) + epsilon) * gain

def rotate(values, positions):
    count, heads_here = (values.shape[0], values.shape[1])
    grid_row = (positions // GRID_W).astype(jnp.float32)
    grid_col = (positions % GRID_W).astype(jnp.float32)
    freqs = HEAD // 4
    inverse = rope_theta ** (-jnp.arange(freqs, dtype=jnp.float32) / freqs)
    angles = jnp.stack([grid_row, grid_col], axis=-1)[:, :, None] * inverse
    cosine = jnp.cos(angles)[:, None]
    sine = jnp.sin(angles)[:, None]
    split = values.reshape(count, heads_here, 2, 2, freqs)
    first_half = split[..., 0, :]
    second_half = split[..., 1, :]
    turned = jnp.stack([first_half * cosine - second_half * sine, first_half * sine + second_half * cosine], axis=-2)
    return turned.reshape(count, heads_here, HEAD)

def reference(latent, context, cond_latent, cond_context, w_shift, w_scale, w_gate, norm_gain, w_query, w_key, w_value, q_gain, k_gain, w_out):
    cond_act = jax.nn.silu(jnp.stack([cond_latent, cond_context]).astype(jnp.float32)).astype(jnp.bfloat16)
    shift = jnp.dot(cond_act, w_shift, preferred_element_type=jnp.float32)
    scale = jnp.dot(cond_act, w_scale, preferred_element_type=jnp.float32)
    gate = jnp.dot(cond_act, w_gate, preferred_element_type=jnp.float32)
    normed = (rms_rows(latent, norm_gain) * (1.0 + scale[0]) + shift[0]).astype(jnp.bfloat16)
    ctx_normed = (rms_rows(context, norm_gain) * (1.0 + scale[1]) + shift[1]).astype(jnp.bfloat16)
    positions = jnp.arange(TOKENS, dtype=jnp.int32)
    group = HEADS // KV_HEADS
    queries = jnp.dot(normed, w_query, preferred_element_type=jnp.float32).reshape(TOKENS, HEADS, HEAD)
    queries = rotate(rms_rows(queries, q_gain), positions).astype(jnp.bfloat16)
    keys = jnp.dot(normed, w_key, preferred_element_type=jnp.float32).reshape(TOKENS, KV_HEADS, HEAD)
    keys = rotate(rms_rows(keys, k_gain), positions).astype(jnp.bfloat16)
    values = jnp.dot(normed, w_value, preferred_element_type=jnp.float32).astype(jnp.bfloat16).reshape(TOKENS, KV_HEADS, HEAD)
    ctx_keys = jnp.dot(ctx_normed, w_key, preferred_element_type=jnp.float32).reshape(CTX, KV_HEADS, HEAD)
    ctx_keys = rms_rows(ctx_keys, k_gain).astype(jnp.bfloat16)
    ctx_values = jnp.dot(ctx_normed, w_value, preferred_element_type=jnp.float32).astype(jnp.bfloat16).reshape(CTX, KV_HEADS, HEAD)
    keys_f = keys.astype(jnp.float32)
    values_f = values.astype(jnp.float32)
    ctx_keys_f = ctx_keys.astype(jnp.float32)
    ctx_values_f = ctx_values.astype(jnp.float32)
    scaling = HEAD ** (-0.5)
    blocks = queries.reshape(TOKENS // TOK_DEV, TOK_DEV, KV_HEADS, group, HEAD)

    def attend(block):
        block_f = block.astype(jnp.float32)
        scores = jnp.einsum('qkgd,skd->kgqs', block_f, keys_f) * scaling
        ctx_scores = jnp.einsum('qkgd,ckd->kgqc', block_f, ctx_keys_f) * scaling + context_lift
        top = jnp.maximum(lax.optimization_barrier(jnp.max(scores, axis=-1)), lax.optimization_barrier(jnp.max(ctx_scores, axis=-1)))
        weights = jnp.exp(scores - top[..., None])
        ctx_weights = jnp.exp(ctx_scores - top[..., None])
        total = lax.optimization_barrier(jnp.sum(weights, axis=-1)) + lax.optimization_barrier(jnp.sum(ctx_weights, axis=-1))
        numerator = jnp.einsum('kgqs,skd->qkgd', weights.astype(jnp.bfloat16).astype(jnp.float32), values_f)
        numerator = numerator + jnp.einsum('kgqc,ckd->qkgd', ctx_weights.astype(jnp.bfloat16).astype(jnp.float32), ctx_values_f)
        return (numerator / jnp.transpose(total, (2, 0, 1))[..., None]).astype(jnp.bfloat16)
    attended = lax.map(attend, blocks).reshape(TOKENS, HEADS * HEAD)
    columns = HEADS * HEAD // N_TP
    heads_out = jnp.zeros((TOKENS, D), jnp.float32)
    for member in range(N_TP):
        partial_out = jnp.dot(attended[:, member * columns:(member + 1) * columns], w_out[member * columns:(member + 1) * columns], preferred_element_type=jnp.float32)
        rounded = lax.optimization_barrier(partial_out.astype(jnp.bfloat16))
        heads_out = heads_out + rounded.astype(jnp.float32)
    return (gate[0] * heads_out).astype(jnp.bfloat16)
```

```python
import functools

import jax
import jax.numpy as jnp
from jax import lax
from jax.experimental import pallas as pl
from jax.experimental.pallas import tpu as pltpu
from jax.sharding import PartitionSpec as P

HEAD = 128
GRID_W = 64
EPS = 1e-06
CONTEXT_LIFT = 1.5
ROPE_THETA = 10000.0
SCALING = HEAD ** -0.5
LOG2E = 1.4426950408889634


BF16 = jnp.bfloat16
F32 = jnp.float32
VM = pl.BlockSpec(memory_space=pltpu.VMEM)


def rotate_rows(v, cos, sin):
    lane = lax.broadcasted_iota(jnp.int32, v.shape, 1)
    quarter = HEAD // 4
    partner = jnp.where(
        lane % (2 * quarter) < quarter,
        pltpu.roll(v, HEAD - quarter, 1),
        pltpu.roll(v, quarter, 1),
    )
    return v * cos + partner * sin


def rms_head(v, gain):
    return v * lax.rsqrt(jnp.mean(v * v, axis=-1, keepdims=True) + EPS) * gain


def kv_kernel(x_ref, c_ref, rx_ref, rc_ref, mod_ref, w_ref, g_ref, cos_ref, sin_ref, kv_ref, nm_ref, cn_ref):
    tok, width = x_ref.shape
    ctx = c_ref.shape[0]
    step = 32

    @pl.loop(0, tok // step)
    def _(i):
        rows = pl.ds(pl.multiple_of(i * step, step), step)
        r = rx_ref[rows, :]
        for j in range(width // 128):
            cs = slice(128 * j, 128 * j + 128)
            v = x_ref[rows, cs].astype(F32) * r
            nm_ref[rows, cs] = (v * mod_ref[0:1, cs] + mod_ref[1:2, cs]).astype(BF16)

    r = rc_ref[...]
    for j in range(width // 128):
        cs = slice(128 * j, 128 * j + 128)
        v = c_ref[:, cs].astype(F32) * r
        cn_ref[:, cs] = (v * mod_ref[2:3, cs] + mod_ref[3:4, cs]).astype(BF16)

    gain = g_ref[...]
    tile = 128

    @pl.loop(0, tok // tile)
    def _(i):
        rows = pl.ds(pl.multiple_of(i * tile, tile), tile)
        both = jnp.dot(nm_ref[rows, :], w_ref[...], preferred_element_type=F32)
        k = rotate_rows(rms_head(both[:, :HEAD], gain), cos_ref[rows, :], sin_ref[rows, :])
        kv_ref[rows, :HEAD] = k.astype(BF16)
        kv_ref[rows, HEAD:] = both[:, HEAD:].astype(BF16)

    both = jnp.dot(cn_ref[...], w_ref[...], preferred_element_type=F32)
    kv_ref[tok:tok + ctx, :HEAD] = rms_head(both[:, :HEAD], gain).astype(BF16)
    kv_ref[tok:tok + ctx, HEAD:] = both[:, HEAD:].astype(BF16)


def q_kernel(nm_ref, w_ref, g_ref, cos_ref, sin_ref, q_ref):
    tok = nm_ref.shape[0]
    heads = w_ref.shape[1] // HEAD
    gain = g_ref[...]
    tile = 128

    @pl.loop(0, tok // tile)
    def _(i):
        rows = pl.ds(pl.multiple_of(i * tile, tile), tile)
        both = jnp.dot(nm_ref[rows, :], w_ref[...], preferred_element_type=F32)
        for h in range(heads):
            v = rotate_rows(rms_head(both[:, h * HEAD:(h + 1) * HEAD], gain), cos_ref[rows, :], sin_ref[rows, :])
            q_ref[pl.ds(pl.multiple_of(h * tok + i * tile, tile), tile), :] = v.astype(BF16)


def attend_block(q_ref, kv_ref, m_ref, l_ref, acc_ref, cols, tok):
    n = kv_ref.shape[0]
    q = q_ref[cols, :]
    s = lax.dot_general(kv_ref[:, :HEAD], q, (((1,), (1,)), ((), ())), preferred_element_type=F32)
    if n > tok:
        s = jnp.concatenate([s[:tok], s[tok:] + CONTEXT_LIFT / SCALING], axis=0)
    old = m_ref[0:1, cols]
    new = jnp.maximum(old, jnp.max(s, axis=0, keepdims=True))
    p = jnp.exp2((s - new) * (SCALING * LOG2E))
    keep = jnp.exp2((old - new) * (SCALING * LOG2E))
    m_ref[0:1, cols] = new
    l_ref[0:1, cols] = l_ref[0:1, cols] * keep + jnp.sum(p, axis=0, keepdims=True)
    o = lax.dot_general(
        kv_ref[:, HEAD:], p.astype(BF16), (((0,), (0,)), ((), ())), preferred_element_type=F32
    )
    acc_ref[:, cols] = acc_ref[:, cols] * keep + o


def attend_kernel(n_kv, first, last, tok, *refs):
    q_ref, kv_refs = refs[0], refs[1:1 + n_kv]
    at = 1 + n_kv
    if not first:
        m_in, l_in, acc_in = refs[at:at + 3]
        at += 3
    if last:
        out_ref = refs[at]
        m_ref, l_ref, acc_ref = refs[at + 1:at + 4]
    else:
        m_ref, l_ref, acc_ref = refs[at:at + 3]
    if first:
        m_ref[...] = jnp.full(m_ref.shape, -1e30, F32)
        l_ref[...] = jnp.zeros(l_ref.shape, F32)
        acc_ref[...] = jnp.zeros(acc_ref.shape, F32)
    else:
        m_ref[...] = m_in[...]
        l_ref[...] = l_in[...]
        acc_ref[...] = acc_in[...]
    queries = q_ref.shape[0]
    width = 256

    @pl.loop(0, queries // width)
    def _(i):
        cols = pl.ds(pl.multiple_of(i * width, width), width)
        for kv_ref in kv_refs:
            attend_block(q_ref, kv_ref, m_ref, l_ref, acc_ref, cols, tok)

    if last:
        for h in range(queries // tok):
            cols = slice(h * tok, (h + 1) * tok)
            done = acc_ref[:, cols] / l_ref[0:1, cols]
            out_ref[:, h * HEAD:(h + 1) * HEAD] = jnp.transpose(done).astype(BF16)


def attend(q, chunks, state, tok, last=False):
    queries = q.shape[0]
    first = state is None
    shapes = [
        jax.ShapeDtypeStruct((8, queries), F32),
        jax.ShapeDtypeStruct((8, queries), F32),
        jax.ShapeDtypeStruct((HEAD, queries), F32),
    ]
    rows = sum(c.shape[0] for c in chunks)
    cost = pl.CostEstimate(
        flops=4 * rows * queries * HEAD, transcendentals=rows * queries, bytes_accessed=1 << 20
    )
    operands = [q, *chunks] + ([] if first else list(state))
    if last:
        return pl.pallas_call(
            functools.partial(attend_kernel, len(chunks), first, True, tok),
            out_shape=jax.ShapeDtypeStruct((tok, queries // tok * HEAD), BF16),
            in_specs=[VM] * len(operands),
            out_specs=VM,
            scratch_shapes=[pltpu.VMEM(s.shape, s.dtype) for s in shapes],
            cost_estimate=cost,
            name="attend_last",
        )(*operands)
    return pl.pallas_call(
        functools.partial(attend_kernel, len(chunks), first, False, tok),
        out_shape=shapes,
        in_specs=[VM] * len(operands),
        out_specs=[VM] * 3,
        input_output_aliases={} if first else {1 + len(chunks) + i: i for i in range(3)},
        cost_estimate=cost,
        name="attend",
    )(*operands)


def copy_for_each(shard, axis):
    copies = jnp.broadcast_to(shard, (lax.axis_size(axis), *shard.shape))
    return lax.all_to_all(copies, axis, split_axis=0, concat_axis=0, tiled=True)


def shifted(x, axis, by):
    n = lax.axis_size(axis)
    return lax.ppermute(x, axis, [(i, (i + by) % n) for i in range(n)])


def other_core(x):
    n = lax.axis_size("tp")
    return lax.ppermute(x, "tp", [(i, i ^ 1) for i in range(n)])


def body(
    latent, context, cond_latent, cond_context, w_shift, w_scale, w_gate, norm_gain,
    w_query, w_key, w_value, q_gain, k_gain, w_out,
):
    seq_index = lax.axis_index("sp")
    n_sp = lax.axis_size("sp")
    tp_index = lax.axis_index("tp")
    mod_rows, mod_cols = w_shift.shape
    tok, width = latent.shape
    ctx = context.shape[0]

    cond_act = jax.nn.silu(jnp.stack([cond_latent, cond_context]).astype(F32)).astype(BF16)
    act_rows = lax.dynamic_slice_in_dim(cond_act, seq_index * mod_rows, mod_rows, 1)
    partial_mod = jnp.concatenate(
        [
            jnp.dot(act_rows, w_scale, preferred_element_type=F32),
            jnp.dot(act_rows, w_shift, preferred_element_type=F32),
            jnp.dot(act_rows, w_gate, preferred_element_type=F32),
        ]
    )
    summed = jnp.sum(copy_for_each(partial_mod, "sp"), axis=0)
    modulation = jnp.moveaxis(copy_for_each(summed, "tp"), 0, 1).reshape(6, width)
    gain = norm_gain * (1.0 + modulation[0:2])
    mods = jnp.stack([gain[0], modulation[2], gain[1], modulation[3]])
    gate = modulation[4]

    def inverse_rms(x):
        x = x.astype(F32)
        r = lax.rsqrt(jnp.mean(x * x, axis=-1, keepdims=True) + EPS)
        return jnp.broadcast_to(r, (x.shape[0], 128))

    rx, rc = inverse_rms(latent), inverse_rms(context)
    w_kv = jnp.concatenate([w_key, w_value], axis=1)
    positions = seq_index * tok + jnp.arange(tok, dtype=jnp.int32)
    freqs = HEAD // 4
    inverse = ROPE_THETA ** (-jnp.arange(freqs, dtype=F32) / freqs)
    row = (positions // GRID_W).astype(F32)[:, None] * inverse
    col = (positions % GRID_W).astype(F32)[:, None] * inverse
    cos = jnp.concatenate([jnp.cos(row), jnp.cos(row), jnp.cos(col), jnp.cos(col)], axis=1)
    sin = jnp.concatenate([-jnp.sin(row), jnp.sin(row), -jnp.sin(col), jnp.sin(col)], axis=1)

    kv, normed = pl.pallas_call(
        kv_kernel,
        out_shape=[
            jax.ShapeDtypeStruct((tok + ctx, 2 * HEAD), BF16),
            jax.ShapeDtypeStruct((tok, width), BF16),
        ],
        in_specs=[VM] * 9,
        out_specs=[VM] * 2,
        scratch_shapes=[pltpu.VMEM((ctx, width), BF16)],
        cost_estimate=pl.CostEstimate(flops=2 * tok * width * 256, transcendentals=0, bytes_accessed=1 << 22),
        name="project_kv",
    )(latent, context, rx, rc, mods, w_kv, k_gain.reshape(1, HEAD), cos, sin)

    right, left = shifted(kv, "sp", 1), shifted(kv, "sp", -1)
    q = pl.pallas_call(
        q_kernel,
        out_shape=jax.ShapeDtypeStruct((w_query.shape[1] // HEAD * tok, HEAD), BF16),
        in_specs=[VM] * 5,
        out_specs=VM,
        cost_estimate=pl.CostEstimate(flops=2 * tok * width * 256, transcendentals=0, bytes_accessed=1 << 22),
        name="project_q",
    )(normed, w_query, q_gain.reshape(1, HEAD), cos, sin)
    state = attend(q, [kv], None, tok)
    half = n_sp // 2
    for step in range(1, half):
        now = [right, left]
        right = shifted(right, "sp", 1)
        if step + 1 < half:
            left = shifted(left, "sp", -1)
        state = attend(q, now, state, tok)
    attended = attend(q, [right], state, tok, last=True)

    n_x = lax.axis_size("tp") // 2
    core, chip = tp_index % 2, tp_index // 2
    share = tok // (2 * n_x)
    parts = attended.reshape(n_x, 2, share, attended.shape[1])
    parts = jnp.concatenate([parts, parts], axis=0)
    parts = lax.dynamic_slice_in_dim(parts, chip, n_x, 0)
    mine = lax.dynamic_index_in_dim(parts, core, 1, keepdims=False).reshape(n_x * share, -1)
    theirs = lax.dynamic_index_in_dim(parts, 1 - core, 1, keepdims=False).reshape(n_x * share, -1)
    sent = other_core(jnp.dot(theirs, w_out, preferred_element_type=F32).astype(BF16))
    total = jnp.dot(mine, w_out, preferred_element_type=F32) + sent.astype(F32)
    blocks = total.reshape(n_x, share, width)
    far = blocks[2].astype(BF16)
    h = width // 2
    from_left = shifted(far[:, :h], "tp", 2)
    from_right = shifted(far[:, h:], "tp", -2)
    nxt = jnp.concatenate([blocks[1][:, :h] + from_left.astype(F32), blocks[1][:, h:]], axis=1).astype(BF16)
    prv = jnp.concatenate([blocks[3][:, :h], blocks[3][:, h:] + from_right.astype(F32)], axis=1).astype(BF16)
    a, b = shifted(nxt, "tp", 2), shifted(prv, "tp", -2)
    heads_out = blocks[0] + a.astype(F32) + b.astype(F32)
    return (gate * heads_out).astype(BF16)


def solution(mesh):
    placed = (
        P(("grp", "sp"), None),
        P(("grp", "sp"), None),
        P("grp"),
        P(),
        P("sp", "tp"),
        P("sp", "tp"),
        P("sp", "tp"),
        P(),
        P(None, "tp"),
        P(None, "tp"),
        P(None, "tp"),
        P(),
        P(),
        P("tp", None),
    )
    return jax.shard_map(
        body, mesh=mesh, in_specs=placed, out_specs=P(("grp", "sp", "tp"), None), check_vma=False
    )
```

```python
import functools

import jax
import jax.numpy as jnp
from jax import lax
from jax.experimental import pallas as pl
from jax.experimental.pallas import tpu as pltpu
from jax.sharding import PartitionSpec as P

HEAD = 128
GRID_W = 64
EPS = 1e-06
CONTEXT_LIFT = 1.5
ROPE_THETA = 10000.0
SCALING = HEAD ** -0.5
LOG2E = 1.4426950408889634


BF16 = jnp.bfloat16
F32 = jnp.float32
VM = pl.BlockSpec(memory_space=pltpu.VMEM)


def rotate_rows(v, cos, sin):
    lane = lax.broadcasted_iota(jnp.int32, v.shape, 1)
    quarter = HEAD // 4
    partner = jnp.where(
        lane % (2 * quarter) < quarter,
        pltpu.roll(v, HEAD - quarter, 1),
        pltpu.roll(v, quarter, 1),
    )
    return v * cos + partner * sin


def rms_head(v, gain):
    return v * lax.rsqrt(jnp.mean(v * v, axis=-1, keepdims=True) + EPS) * gain


def modulation_kernel(act_ref, scale_hbm, shift_hbm, gate_hbm, out_ref, w_ref, sems):
    copies = [
        pltpu.make_async_copy(w, w_ref.at[i], sems.at[i])
        for i, w in enumerate((scale_hbm, shift_hbm, gate_hbm))
    ]
    for c in copies:
        c.start()
    act = act_ref[...]
    pieces = w_ref.shape[2] // 128
    rows = []
    for i, c in enumerate(copies):
        c.wait()
        part = jnp.dot(act, w_ref[i], preferred_element_type=F32)
        rows += [part[0:1], part[1:2]] if i < 2 else [part[0:1]]
    tile = jnp.concatenate(
        [r[:, 128 * j:128 * j + 128] for r in rows for j in range(pieces)]
        + [jnp.zeros((out_ref.shape[1] - pieces * len(rows), 128), F32)],
        axis=0,
    )
    for i in range(out_ref.shape[0]):
        out_ref[i] = tile


def sum_kernel(in_ref, out_ref):
    total = in_ref[0]
    for i in range(1, in_ref.shape[0]):
        total = total + in_ref[i]
    out_ref[...] = total


def prepare_kernel(x_ref, c_ref, wk_ref, wv_ref, rx_ref, rc_ref, w_ref):
    tok, width = x_ref.shape
    step = 16

    def rows_of(src, dst, rows):
        total = jnp.zeros((step, 128), F32)
        for j in range(width // 128):
            v = src[rows, 128 * j:128 * j + 128].astype(F32)
            total = total + v * v
        r = lax.rsqrt(jnp.sum(total, axis=-1, keepdims=True) / width + EPS)
        dst[rows, :] = jnp.broadcast_to(r, (step, 128))

    @pl.loop(0, tok // step)
    def _(i):
        rows_of(x_ref, rx_ref, pl.ds(pl.multiple_of(i * step, step), step))

    for i in range(c_ref.shape[0] // step):
        rows_of(c_ref, rc_ref, pl.ds(i * step, step))

    @pl.loop(0, w_ref.shape[0] // 256)
    def _(i):
        rows = pl.ds(pl.multiple_of(i * 256, 256), 256)
        w_ref[rows, :HEAD] = wk_ref[rows, :]
        w_ref[rows, HEAD:] = wv_ref[rows, :]


def kv_kernel(
    x_ref, c_ref, rx_ref, rc_ref, own_ref, m1_ref, m3_ref, m2_ref, gain_ref, w_ref, g_ref, cos_ref, sin_ref,
    kv_ref, nm_ref, gate_ref, cn_ref, mod_ref, ab_ref,
):
    tok, width = x_ref.shape
    ctx = c_ref.shape[0]
    n_tp = lax.axis_size("tp")
    chip, core = lax.axis_index("tp") // 2, lax.axis_index("tp") % 2
    n_x = n_tp // 2
    for back, ref in ((0, own_ref), (1, m1_ref), (3, m3_ref), (2, m2_ref)):
        source = lax.rem(chip + n_x - back, n_x)
        for c in range(2):
            mod_ref[2 * source + lax.rem(core + c, 2)] = ref[c]
    pieces = width // n_tp // 128
    for t in range(n_tp):
        for p in range(pieces):
            cs = slice((t * pieces + p) * 128, (t * pieces + p + 1) * 128)
            for row in range(2):
                at = row * pieces + p
                ab_ref[2 * row:2 * row + 1, cs] = gain_ref[:, cs] * (1.0 + mod_ref[t, at:at + 1, :])
                at = (2 + row) * pieces + p
                ab_ref[2 * row + 1:2 * row + 2, cs] = mod_ref[t, at:at + 1, :]
            gate_ref[:, cs] = mod_ref[t, 4 * pieces + p:4 * pieces + p + 1, :]

    step = 64

    @pl.loop(0, tok // step)
    def _(i):
        rows = pl.ds(pl.multiple_of(i * step, step), step)
        r = rx_ref[rows, :]
        for j in range(width // 128):
            cs = slice(128 * j, 128 * j + 128)
            v = x_ref[rows, cs].astype(F32) * r
            nm_ref[rows, cs] = (v * ab_ref[0:1, cs] + ab_ref[1:2, cs]).astype(BF16)

    r = rc_ref[...]
    for j in range(width // 128):
        cs = slice(128 * j, 128 * j + 128)
        cn_ref[:, cs] = (c_ref[:, cs].astype(F32) * r * ab_ref[2:3, cs] + ab_ref[3:4, cs]).astype(BF16)

    gain = g_ref[...]
    tile = 128

    @pl.loop(0, tok // tile)
    def _(i):
        rows = pl.ds(pl.multiple_of(i * tile, tile), tile)
        both = jnp.dot(nm_ref[rows, :], w_ref[...], preferred_element_type=F32)
        k = rotate_rows(rms_head(both[:, :HEAD], gain), cos_ref[rows, :], sin_ref[rows, :])
        kv_ref[rows, :HEAD] = k.astype(BF16)
        kv_ref[rows, HEAD:] = both[:, HEAD:].astype(BF16)

    both = jnp.dot(cn_ref[...], w_ref[...], preferred_element_type=F32)
    kv_ref[tok:tok + ctx, :HEAD] = rms_head(both[:, :HEAD], gain).astype(BF16)
    kv_ref[tok:tok + ctx, HEAD:] = both[:, HEAD:].astype(BF16)


def q_kernel(nm_ref, w_ref, g_ref, cos_ref, sin_ref, q_ref):
    tok = nm_ref.shape[0]
    heads = w_ref.shape[1] // HEAD
    gain = g_ref[...]
    tile = 128

    @pl.loop(0, tok // tile)
    def _(i):
        rows = pl.ds(pl.multiple_of(i * tile, tile), tile)
        both = jnp.dot(nm_ref[rows, :], w_ref[...], preferred_element_type=F32)
        for h in range(heads):
            v = rotate_rows(rms_head(both[:, h * HEAD:(h + 1) * HEAD], gain), cos_ref[rows, :], sin_ref[rows, :])
            q_ref[pl.ds(pl.multiple_of(h * tok + i * tile, tile), tile), :] = v.astype(BF16)


def attend_block(q_ref, kv_ref, m_ref, l_ref, acc_ref, cols, tok):
    n = kv_ref.shape[0]
    q = q_ref[cols, :]
    s = lax.dot_general(kv_ref[:, :HEAD], q, (((1,), (1,)), ((), ())), preferred_element_type=F32)
    if n > tok:
        s = jnp.concatenate([s[:tok], s[tok:] + CONTEXT_LIFT / SCALING], axis=0)
    old = m_ref[0:1, cols]
    new = jnp.maximum(old, jnp.max(s, axis=0, keepdims=True))
    p = jnp.exp2((s - new) * (SCALING * LOG2E))
    keep = jnp.exp2((old - new) * (SCALING * LOG2E))
    m_ref[0:1, cols] = new
    l_ref[0:1, cols] = l_ref[0:1, cols] * keep + jnp.sum(p, axis=0, keepdims=True)
    o = lax.dot_general(
        kv_ref[:, HEAD:], p.astype(BF16), (((0,), (0,)), ((), ())), preferred_element_type=F32
    )
    acc_ref[:, cols] = acc_ref[:, cols] * keep + o


def attend_kernel(n_kv, first, last, tok, *refs):
    q_ref, kv_refs = refs[0], refs[1:1 + n_kv]
    at = 1 + n_kv
    if not first:
        m_in, l_in, acc_in = refs[at:at + 3]
        at += 3
    if last:
        out_ref = refs[at]
        m_ref, l_ref, acc_ref = refs[at + 1:at + 4]
    else:
        m_ref, l_ref, acc_ref = refs[at:at + 3]
    if first:
        m_ref[...] = jnp.full(m_ref.shape, -1e30, F32)
        l_ref[...] = jnp.zeros(l_ref.shape, F32)
        acc_ref[...] = jnp.zeros(acc_ref.shape, F32)
    else:
        m_ref[...] = m_in[...]
        l_ref[...] = l_in[...]
        acc_ref[...] = acc_in[...]
    queries = q_ref.shape[0]
    width = 256

    @pl.loop(0, queries // width)
    def _(i):
        cols = pl.ds(pl.multiple_of(i * width, width), width)
        for kv_ref in kv_refs:
            attend_block(q_ref, kv_ref, m_ref, l_ref, acc_ref, cols, tok)

    if last:
        for h in range(queries // tok):
            cols = slice(h * tok, (h + 1) * tok)
            done = acc_ref[:, cols] / l_ref[0:1, cols]
            out_ref[:, h * HEAD:(h + 1) * HEAD] = jnp.transpose(done).astype(BF16)


def attend(q, chunks, state, tok, last=False):
    queries = q.shape[0]
    first = state is None
    shapes = [
        jax.ShapeDtypeStruct((8, queries), F32),
        jax.ShapeDtypeStruct((8, queries), F32),
        jax.ShapeDtypeStruct((HEAD, queries), F32),
    ]
    rows = sum(c.shape[0] for c in chunks)
    cost = pl.CostEstimate(
        flops=4 * rows * queries * HEAD, transcendentals=rows * queries, bytes_accessed=1 << 20
    )
    operands = [q, *chunks] + ([] if first else list(state))
    if last:
        return pl.pallas_call(
            functools.partial(attend_kernel, len(chunks), first, True, tok),
            out_shape=jax.ShapeDtypeStruct((tok, queries // tok * HEAD), BF16),
            in_specs=[VM] * len(operands),
            out_specs=VM,
            scratch_shapes=[pltpu.VMEM(s.shape, s.dtype) for s in shapes],
            cost_estimate=cost,
            compiler_params=pltpu.CompilerParams(vmem_limit_bytes=16 << 20),
            name="attend_last",
        )(*operands)
    return pl.pallas_call(
        functools.partial(attend_kernel, len(chunks), first, False, tok),
        out_shape=shapes,
        in_specs=[VM] * len(operands),
        out_specs=[VM] * 3,
        input_output_aliases={} if first else {1 + len(chunks) + i: i for i in range(3)},
        cost_estimate=cost,
        compiler_params=pltpu.CompilerParams(vmem_limit_bytes=16 << 20),
        name="attend",
    )(*operands)


def shifted(x, axis, by):
    n = lax.axis_size(axis)
    return lax.ppermute(x, axis, [(i, (i + by) % n) for i in range(n)])


def other_core(x):
    n = lax.axis_size("tp")
    return lax.ppermute(x, "tp", [(i, i ^ 1) for i in range(n)])


def body(
    latent, context, cond_latent, cond_context, w_shift, w_scale, w_gate, norm_gain,
    w_query, w_key, w_value, q_gain, k_gain, w_out,
):
    seq_index = lax.axis_index("sp")
    n_sp = lax.axis_size("sp")
    tp_index = lax.axis_index("tp")
    mod_rows, mod_cols = w_shift.shape
    tok, width = latent.shape
    ctx = context.shape[0]

    act_rows = jnp.stack(
        [
            jax.nn.silu(lax.dynamic_slice_in_dim(c, seq_index * mod_rows, mod_rows).astype(F32)).astype(BF16)
            for c in (cond_latent, cond_context)
        ]
    )
    n_tp = lax.axis_size("tp")
    pieces = mod_cols // 128
    lines = -(-5 * pieces // 8) * 8
    partial_mod = pl.pallas_call(
        modulation_kernel,
        out_shape=jax.ShapeDtypeStruct((n_sp, lines, 128), F32),
        in_specs=[VM] + [pl.BlockSpec(memory_space=pltpu.HBM)] * 3,
        out_specs=VM,
        scratch_shapes=[pltpu.VMEM((3, mod_rows, mod_cols), BF16), pltpu.SemaphoreType.DMA((3,))],
        compiler_params=pltpu.CompilerParams(vmem_limit_bytes=8 << 20),
        name="modulation",
    )(act_rows, w_scale, w_shift, w_gate)
    gathered = lax.all_to_all(partial_mod, "sp", split_axis=0, concat_axis=0, tiled=True)
    rx, rc, w_kv = pl.pallas_call(
        prepare_kernel,
        out_shape=[
            jax.ShapeDtypeStruct((tok, 128), F32),
            jax.ShapeDtypeStruct((ctx, 128), F32),
            jax.ShapeDtypeStruct((width, 2 * HEAD), BF16),
        ],
        in_specs=[VM] * 4,
        out_specs=[VM] * 3,
        compiler_params=pltpu.CompilerParams(vmem_limit_bytes=32 << 20),
        cost_estimate=pl.CostEstimate(flops=1 << 30, transcendentals=0, bytes_accessed=12 << 20),
        name="prepare",
    )(latent, context, w_key, w_value)
    positions = seq_index * tok + jnp.arange(tok, dtype=jnp.int32)
    freqs = HEAD // 4
    inverse = ROPE_THETA ** (-jnp.arange(freqs, dtype=F32) / freqs)
    row = (positions // GRID_W).astype(F32)[:, None] * inverse
    col = (positions % GRID_W).astype(F32)[:, None] * inverse
    cos = jnp.concatenate([jnp.cos(row), jnp.cos(row), jnp.cos(col), jnp.cos(col)], axis=1)
    sin = jnp.concatenate([-jnp.sin(row), jnp.sin(row), -jnp.sin(col), jnp.sin(col)], axis=1)

    gathered, rx, rc, w_kv, cos, sin = lax.optimization_barrier((gathered, rx, rc, w_kv, cos, sin))
    summed = pl.pallas_call(
        sum_kernel,
        out_shape=jax.ShapeDtypeStruct((lines, 128), F32),
        in_specs=[VM],
        out_specs=VM,
        compiler_params=pltpu.CompilerParams(vmem_limit_bytes=8 << 20),
        name="sum_parts",
    )(gathered)
    pair = jnp.stack([summed, other_core(summed)])
    columns = [pair, shifted(pair, "tp", 2), shifted(pair, "tp", -2), shifted(pair, "tp", 4)]

    kv, normed, gate = pl.pallas_call(
        kv_kernel,
        out_shape=[
            jax.ShapeDtypeStruct((tok + ctx, 2 * HEAD), BF16),
            jax.ShapeDtypeStruct((tok, width), BF16),
            jax.ShapeDtypeStruct((1, width), F32),
        ],
        in_specs=[VM] * 13,
        out_specs=[VM] * 3,
        scratch_shapes=[
            pltpu.VMEM((ctx, width), BF16),
            pltpu.VMEM((n_tp, lines, 128), F32),
            pltpu.VMEM((8, width), F32),
        ],
        cost_estimate=pl.CostEstimate(flops=2 * tok * width * 256, transcendentals=0, bytes_accessed=1 << 22),
        compiler_params=pltpu.CompilerParams(vmem_limit_bytes=24 << 20),
        name="project_kv",
    )(
        latent, context, rx, rc, *columns, norm_gain.reshape(1, width), w_kv, k_gain.reshape(1, HEAD), cos, sin
    )

    right, left = shifted(kv, "sp", 1), shifted(kv, "sp", -1)
    q = pl.pallas_call(
        q_kernel,
        out_shape=jax.ShapeDtypeStruct((w_query.shape[1] // HEAD * tok, HEAD), BF16),
        in_specs=[VM] * 5,
        out_specs=VM,
        cost_estimate=pl.CostEstimate(flops=2 * tok * width * 256, transcendentals=0, bytes_accessed=1 << 22),
        compiler_params=pltpu.CompilerParams(vmem_limit_bytes=24 << 20),
        name="project_q",
    )(normed, w_query, q_gain.reshape(1, HEAD), cos, sin)
    state = attend(q, [kv], None, tok)
    half = n_sp // 2
    for step in range(1, half):
        right, left, m = lax.optimization_barrier((right, left, state[0]))
        state = [m, *state[1:]]
        now = [right, left]
        right = shifted(right, "sp", 1)
        if step + 1 < half:
            left = shifted(left, "sp", -1)
        state = attend(q, now, state, tok)
    attended = attend(q, [right], state, tok, last=True)

    n_x = lax.axis_size("tp") // 2
    core, chip = tp_index % 2, tp_index // 2
    share = tok // (2 * n_x)
    parts = attended.reshape(n_x, 2, share, attended.shape[1])
    parts = jnp.concatenate([parts, parts], axis=0)
    parts = lax.dynamic_slice_in_dim(parts, chip, n_x, 0)
    mine = lax.dynamic_index_in_dim(parts, core, 1, keepdims=False).reshape(n_x * share, -1)
    theirs = lax.dynamic_index_in_dim(parts, 1 - core, 1, keepdims=False).reshape(n_x * share, -1)
    sent = other_core(jnp.dot(theirs, w_out, preferred_element_type=F32).astype(BF16))
    total = jnp.dot(mine, w_out, preferred_element_type=F32) + sent.astype(F32)
    blocks = total.reshape(n_x, share, width)
    far = blocks[2].astype(BF16)
    h = width // 2
    from_left = shifted(far[:, :h], "tp", 2)
    from_right = shifted(far[:, h:], "tp", -2)
    nxt = jnp.concatenate([blocks[1][:, :h] + from_left.astype(F32), blocks[1][:, h:]], axis=1).astype(BF16)
    prv = jnp.concatenate([blocks[3][:, :h], blocks[3][:, h:] + from_right.astype(F32)], axis=1).astype(BF16)
    a, b = shifted(nxt, "tp", 2), shifted(prv, "tp", -2)
    heads_out = blocks[0] + a.astype(F32) + b.astype(F32)
    return (gate * heads_out).astype(BF16)


def solution(mesh):
    placed = (
        P(("grp", "sp"), None),
        P(("grp", "sp"), None),
        P("grp"),
        P(),
        P("sp", "tp"),
        P("sp", "tp"),
        P("sp", "tp"),
        P(),
        P(None, "tp"),
        P(None, "tp"),
        P(None, "tp"),
        P(),
        P(),
        P("tp", None),
    )
    return jax.shard_map(
        body, mesh=mesh, in_specs=placed, out_specs=P(("grp", "sp", "tp"), None), check_vma=False
    )
```

```python
import functools

import jax
import jax.numpy as jnp
from jax import lax
from jax.experimental import pallas as pl
from jax.experimental.pallas import tpu as pltpu
from jax.sharding import PartitionSpec as P

HEAD = 128
GRID_W = 64
EPS = 1e-06
CONTEXT_LIFT = 1.5
ROPE_THETA = 10000.0
SCALING = HEAD ** -0.5
LOG2E = 1.4426950408889634


BF16 = jnp.bfloat16
F32 = jnp.float32
VM = pl.BlockSpec(memory_space=pltpu.VMEM)


def rotate_rows(v, cos, sin):
    lane = lax.broadcasted_iota(jnp.int32, v.shape, 1)
    quarter = HEAD // 4
    partner = jnp.where(
        lane % (2 * quarter) < quarter,
        pltpu.roll(v, HEAD - quarter, 1),
        pltpu.roll(v, quarter, 1),
    )
    return v * cos + partner * sin


def rms_head(v, gain):
    return v * lax.rsqrt(jnp.mean(v * v, axis=-1, keepdims=True) + EPS) * gain


def modulation_kernel(lat_ref, ctx_ref, scale_hbm, shift_hbm, gate_hbm, out_ref, w_ref, sems):
    copies = [
        pltpu.make_async_copy(w, w_ref.at[i], sems.at[i])
        for i, w in enumerate((scale_hbm, shift_hbm, gate_hbm))
    ]
    for c in copies:
        c.start()
    act = jnp.concatenate([lat_ref[...], ctx_ref[...]], axis=0)
    pieces = w_ref.shape[2] // 128
    rows, context_rows = [], []
    for i, c in enumerate(copies):
        c.wait()
        part = jnp.dot(act, w_ref[i], preferred_element_type=F32)
        near = part[0:1].astype(BF16).astype(F32)
        rows += [near, part[0:1] - near]
        if i < 2:
            context_rows.append(part[1:2])
    tile = jnp.concatenate(
        [r[:, 128 * j:128 * j + 128] for r in rows + context_rows for j in range(pieces)], axis=0
    ).astype(BF16)
    for i in range(out_ref.shape[0]):
        out_ref[i] = tile


def sum_kernel(in_ref, out_ref):
    total = in_ref[0].astype(F32)
    for i in range(1, in_ref.shape[0]):
        total = total + in_ref[i].astype(F32)
    pieces = in_ref.shape[1] // 8
    for i in range(3):
        at = 2 * i * pieces
        out_ref[i * pieces:(i + 1) * pieces, :] = total[at:at + pieces] + total[at + pieces:at + 2 * pieces]
    out_ref[3 * pieces:5 * pieces, :] = total[6 * pieces:8 * pieces]
    out_ref[5 * pieces:, :] = jnp.zeros((out_ref.shape[0] - 5 * pieces, 128), F32)


def prepare_kernel(x_ref, c_ref, wk_ref, wv_ref, rx_ref, rc_ref, w_ref):
    tok, width = x_ref.shape
    step = 16

    def rows_of(src, dst, rows):
        total = jnp.zeros((step, 128), F32)
        for j in range(width // 128):
            v = src[rows, 128 * j:128 * j + 128].astype(F32)
            total = total + v * v
        r = lax.rsqrt(jnp.sum(total, axis=-1, keepdims=True) / width + EPS)
        dst[rows, :] = jnp.broadcast_to(r, (step, 128))

    @pl.loop(0, tok // step)
    def _(i):
        rows_of(x_ref, rx_ref, pl.ds(pl.multiple_of(i * step, step), step))

    for i in range(c_ref.shape[0] // step):
        rows_of(c_ref, rc_ref, pl.ds(i * step, step))

    @pl.loop(0, w_ref.shape[0] // 256)
    def _(i):
        rows = pl.ds(pl.multiple_of(i * 256, 256), 256)
        w_ref[rows, :HEAD] = wk_ref[rows, :]
        w_ref[rows, HEAD:] = wv_ref[rows, :]


def kv_kernel(
    x_ref, c_ref, rx_ref, rc_ref, own_ref, m1_ref, m3_ref, m2_ref, gain_ref, w_ref, g_ref, cos_ref, sin_ref,
    kv_ref, nm_ref, gate_ref, both_ref, mod_ref, ab_ref,
):
    tok, width = x_ref.shape
    ctx = c_ref.shape[0]
    n_tp = lax.axis_size("tp")
    chip, core = lax.axis_index("tp") // 2, lax.axis_index("tp") % 2
    n_x = n_tp // 2
    for back, ref in ((0, own_ref), (1, m1_ref), (3, m3_ref), (2, m2_ref)):
        source = lax.rem(chip + n_x - back, n_x)
        for c in range(2):
            mod_ref[2 * source + lax.rem(core + c, 2)] = ref[c]
    pieces = width // n_tp // 128
    for t in range(n_tp):
        for p in range(pieces):
            cs = slice((t * pieces + p) * 128, (t * pieces + p + 1) * 128)
            piece = [mod_ref[t, i * pieces + p:i * pieces + p + 1, :] for i in range(5)]
            gain = gain_ref[:, cs]
            ab_ref[0:1, cs] = gain * (1.0 + piece[0])
            ab_ref[1:2, cs] = piece[1]
            gate_ref[:, cs] = piece[2]
            ab_ref[2:3, cs] = gain * (1.0 + piece[3])
            ab_ref[3:4, cs] = piece[4]

    step = 64

    @pl.loop(0, tok // step)
    def _(i):
        rows = pl.ds(pl.multiple_of(i * step, step), step)
        r = rx_ref[rows, :]
        for j in range(width // 128):
            cs = slice(128 * j, 128 * j + 128)
            v = x_ref[rows, cs].astype(F32) * r
            nm_ref[rows, cs] = (v * ab_ref[0:1, cs] + ab_ref[1:2, cs]).astype(BF16)

    r = rc_ref[...]
    for j in range(width // 128):
        cs = slice(128 * j, 128 * j + 128)
        nm_ref[tok:tok + ctx, cs] = (c_ref[:, cs].astype(F32) * r * ab_ref[2:3, cs] + ab_ref[3:4, cs]).astype(BF16)

    both_ref[...] = jnp.dot(nm_ref[...], w_ref[...], preferred_element_type=F32)
    kv_ref[:, HEAD:] = both_ref[:, HEAD:].astype(BF16)
    gain = g_ref[...]
    tile = 128

    @pl.loop(0, tok // tile)
    def _(i):
        rows = pl.ds(pl.multiple_of(i * tile, tile), tile)
        k = rotate_rows(rms_head(both_ref[rows, :HEAD], gain), cos_ref[rows, :], sin_ref[rows, :])
        kv_ref[rows, :HEAD] = k.astype(BF16)

    kv_ref[tok:tok + ctx, :HEAD] = rms_head(both_ref[tok:tok + ctx, :HEAD], gain).astype(BF16)


def q_kernel(nm_ref, w_ref, g_ref, cos_ref, sin_ref, q_ref, both_ref):
    tok = cos_ref.shape[0]
    heads = w_ref.shape[1] // HEAD
    gain = g_ref[...]
    tile = 128
    both_ref[...] = jnp.dot(nm_ref[:tok, :], w_ref[...], preferred_element_type=F32)

    @pl.loop(0, tok // tile)
    def _(i):
        rows = pl.ds(pl.multiple_of(i * tile, tile), tile)
        for h in range(heads):
            v = rotate_rows(
                rms_head(both_ref[rows, h * HEAD:(h + 1) * HEAD], gain), cos_ref[rows, :], sin_ref[rows, :]
            )
            q_ref[pl.ds(pl.multiple_of(h * tok + i * tile, tile), tile), :] = v.astype(BF16)


def attend_block(q_ref, kv_refs, vt_ref, m_ref, l_ref, acc_ref, cols, tok):
    q = q_ref[cols, :]
    scores = []
    for kv_ref in kv_refs:
        s = lax.dot_general(kv_ref[:, :HEAD], q, (((1,), (1,)), ((), ())), preferred_element_type=F32)
        scores += [s[:tok], s[tok:] + CONTEXT_LIFT / SCALING]
    old = m_ref[0:1, cols]
    new = old
    for s in scores:
        new = jnp.maximum(new, jnp.max(s, axis=0, keepdims=True))
    keep = jnp.exp2((old - new) * (SCALING * LOG2E))
    m_ref[0:1, cols] = new
    total = l_ref[0:1, cols] * keep
    out = acc_ref[:, cols] * keep
    for i in range(len(kv_refs)):
        p = jnp.exp2((jnp.concatenate(scores[2 * i:2 * i + 2], axis=0) - new) * (SCALING * LOG2E))
        total = total + jnp.sum(p, axis=0, keepdims=True)
        out = out + jnp.dot(vt_ref[i], p.astype(BF16), preferred_element_type=F32)
    l_ref[0:1, cols] = total
    acc_ref[:, cols] = out


def attend_kernel(n_kv, first, last, tok, *refs):
    q_ref, kv_refs = refs[0], refs[1:1 + n_kv]
    at = 1 + n_kv
    if not first:
        m_in, l_in, acc_in = refs[at:at + 3]
        at += 3
    if last:
        out_ref = refs[at]
        at += 1
        m_ref, l_ref, acc_ref = refs[at + 1:at + 4]
        vt_ref = refs[at]
    else:
        m_ref, l_ref, acc_ref = refs[at:at + 3]
        vt_ref = refs[at + 3]
    if first:
        m_ref[...] = jnp.full(m_ref.shape, -1e30, F32)
        l_ref[...] = jnp.zeros(l_ref.shape, F32)
        acc_ref[...] = jnp.zeros(acc_ref.shape, F32)
    else:
        m_ref[...] = m_in[...]
        l_ref[...] = l_in[...]
        acc_ref[...] = acc_in[...]
    for i, kv_ref in enumerate(kv_refs):
        vt_ref[i] = jnp.transpose(kv_ref[:, HEAD:])
    queries = q_ref.shape[0]
    width = 256

    @pl.loop(0, queries // width)
    def _(i):
        cols = pl.ds(pl.multiple_of(i * width, width), width)
        attend_block(q_ref, kv_refs, vt_ref, m_ref, l_ref, acc_ref, cols, tok)

    if last:
        for h in range(queries // tok):
            cols = slice(h * tok, (h + 1) * tok)
            done = acc_ref[:, cols] / l_ref[0:1, cols]
            out_ref[:, h * HEAD:(h + 1) * HEAD] = jnp.transpose(done).astype(BF16)


def attend(q, chunks, state, tok, last=False):
    queries = q.shape[0]
    first = state is None
    shapes = [
        jax.ShapeDtypeStruct((8, queries), F32),
        jax.ShapeDtypeStruct((8, queries), F32),
        jax.ShapeDtypeStruct((HEAD, queries), F32),
    ]
    rows = sum(c.shape[0] for c in chunks)
    turned = pltpu.VMEM((len(chunks), HEAD, chunks[0].shape[0]), BF16)
    cost = pl.CostEstimate(
        flops=4 * rows * queries * HEAD, transcendentals=rows * queries, bytes_accessed=1 << 20
    )
    operands = [q, *chunks] + ([] if first else list(state))
    if last:
        return pl.pallas_call(
            functools.partial(attend_kernel, len(chunks), first, True, tok),
            out_shape=jax.ShapeDtypeStruct((tok, queries // tok * HEAD), BF16),
            in_specs=[VM] * len(operands),
            out_specs=VM,
            scratch_shapes=[turned, *[pltpu.VMEM(s.shape, s.dtype) for s in shapes]],
            cost_estimate=cost,
            compiler_params=pltpu.CompilerParams(vmem_limit_bytes=16 << 20),
            name="attend_last",
        )(*operands)
    return pl.pallas_call(
        functools.partial(attend_kernel, len(chunks), first, False, tok),
        out_shape=shapes,
        in_specs=[VM] * len(operands),
        out_specs=[VM] * 3,
        scratch_shapes=[turned],
        input_output_aliases={} if first else {1 + len(chunks) + i: i for i in range(3)},
        cost_estimate=cost,
        compiler_params=pltpu.CompilerParams(vmem_limit_bytes=16 << 20),
        name="attend",
    )(*operands)


def shifted(x, axis, by):
    n = lax.axis_size(axis)
    return lax.ppermute(x, axis, [(i, (i + by) % n) for i in range(n)])


def other_core(x):
    n = lax.axis_size("tp")
    return lax.ppermute(x, "tp", [(i, i ^ 1) for i in range(n)])


def body(
    latent, context, cond_latent, cond_context, w_shift, w_scale, w_gate, norm_gain,
    w_query, w_key, w_value, q_gain, k_gain, w_out,
):
    seq_index = lax.axis_index("sp")
    n_sp = lax.axis_size("sp")
    tp_index = lax.axis_index("tp")
    mod_rows, mod_cols = w_shift.shape
    tok, width = latent.shape
    ctx = context.shape[0]

    act_rows = [
        jax.nn.silu(lax.dynamic_slice_in_dim(c, seq_index * mod_rows, mod_rows).astype(F32))
        .astype(BF16)
        .reshape(1, mod_rows)
        for c in (cond_latent, cond_context)
    ]
    n_tp = lax.axis_size("tp")
    pieces = mod_cols // 128
    lines = -(-5 * pieces // 8) * 8
    partial_mod = pl.pallas_call(
        modulation_kernel,
        out_shape=jax.ShapeDtypeStruct((n_sp, 8 * pieces, 128), BF16),
        in_specs=[VM] * 2 + [pl.BlockSpec(memory_space=pl.ANY)] * 3,
        out_specs=VM,
        scratch_shapes=[pltpu.VMEM((3, mod_rows, mod_cols), BF16), pltpu.SemaphoreType.DMA((3,))],
        compiler_params=pltpu.CompilerParams(vmem_limit_bytes=60 << 20),
        name="modulation",
    )(*act_rows, w_scale, w_shift, w_gate)
    gathered = lax.all_to_all(partial_mod, "sp", split_axis=0, concat_axis=0, tiled=True)
    rx, rc, w_kv = pl.pallas_call(
        prepare_kernel,
        out_shape=[
            jax.ShapeDtypeStruct((tok, 128), F32),
            jax.ShapeDtypeStruct((ctx, 128), F32),
            jax.ShapeDtypeStruct((width, 2 * HEAD), BF16),
        ],
        in_specs=[VM] * 4,
        out_specs=[VM] * 3,
        compiler_params=pltpu.CompilerParams(vmem_limit_bytes=32 << 20),
        cost_estimate=pl.CostEstimate(flops=1 << 30, transcendentals=0, bytes_accessed=12 << 20),
        name="prepare",
    )(latent, context, w_key, w_value)
    positions = seq_index * tok + jnp.arange(tok, dtype=jnp.int32)
    freqs = HEAD // 4
    inverse = ROPE_THETA ** (-jnp.arange(freqs, dtype=F32) / freqs)
    row = (positions // GRID_W).astype(F32)[:, None] * inverse
    col = (positions % GRID_W).astype(F32)[:, None] * inverse
    cos = jnp.concatenate([jnp.cos(row), jnp.cos(row), jnp.cos(col), jnp.cos(col)], axis=1)
    sin = jnp.concatenate([-jnp.sin(row), jnp.sin(row), -jnp.sin(col), jnp.sin(col)], axis=1)

    gathered, rx, rc, w_kv, cos, sin = lax.optimization_barrier((gathered, rx, rc, w_kv, cos, sin))
    summed = pl.pallas_call(
        sum_kernel,
        out_shape=jax.ShapeDtypeStruct((lines, 128), F32),
        in_specs=[VM],
        out_specs=VM,
        compiler_params=pltpu.CompilerParams(vmem_limit_bytes=8 << 20),
        cost_estimate=pl.CostEstimate(flops=8 << 30, transcendentals=0, bytes_accessed=1 << 20),
        name="sum_parts",
    )(gathered)
    pair = jnp.stack([summed, other_core(summed)])
    columns = [pair, shifted(pair, "tp", 2), shifted(pair, "tp", -2), shifted(pair, "tp", 4)]

    kv, normed, gate = pl.pallas_call(
        kv_kernel,
        out_shape=[
            jax.ShapeDtypeStruct((tok + ctx, 2 * HEAD), BF16),
            jax.ShapeDtypeStruct((tok + ctx, width), BF16),
            jax.ShapeDtypeStruct((1, width), F32),
        ],
        in_specs=[VM] * 13,
        out_specs=[VM] * 3,
        scratch_shapes=[
            pltpu.VMEM((tok + ctx, 2 * HEAD), F32),
            pltpu.VMEM((n_tp, lines, 128), F32),
            pltpu.VMEM((8, width), F32),
        ],
        cost_estimate=pl.CostEstimate(flops=2 * tok * width * 256, transcendentals=0, bytes_accessed=1 << 22),
        compiler_params=pltpu.CompilerParams(vmem_limit_bytes=24 << 20),
        name="project_kv",
    )(
        latent, context, rx, rc, *columns, norm_gain.reshape(1, width), w_kv, k_gain.reshape(1, HEAD), cos, sin
    )

    right, left = shifted(kv, "sp", 1), shifted(kv, "sp", -1)
    q = pl.pallas_call(
        q_kernel,
        out_shape=jax.ShapeDtypeStruct((w_query.shape[1] // HEAD * tok, HEAD), BF16),
        in_specs=[VM] * 5,
        out_specs=VM,
        scratch_shapes=[pltpu.VMEM((tok, w_query.shape[1]), F32)],
        cost_estimate=pl.CostEstimate(flops=2 * tok * width * 256, transcendentals=0, bytes_accessed=1 << 22),
        compiler_params=pltpu.CompilerParams(vmem_limit_bytes=24 << 20),
        name="project_q",
    )(normed, w_query, q_gain.reshape(1, HEAD), cos, sin)
    state = attend(q, [kv], None, tok)
    half = n_sp // 2
    for step in range(1, half):
        right, m = lax.optimization_barrier((right, state[0]))
        left, m = lax.optimization_barrier((left, m))
        state = [m, *state[1:]]
        now = [right, left]
        right = shifted(right, "sp", 1)
        if step + 1 < half:
            left = shifted(left, "sp", -1)
        state = attend(q, now, state, tok)
    attended = attend(q, [right], state, tok, last=True)

    n_x = lax.axis_size("tp") // 2
    core, chip = tp_index % 2, tp_index // 2
    share = tok // (2 * n_x)
    parts = attended.reshape(n_x, 2, share, attended.shape[1])
    parts = jnp.concatenate([parts, parts], axis=0)
    parts = lax.dynamic_slice_in_dim(parts, chip, n_x, 0)
    mine = lax.dynamic_index_in_dim(parts, core, 1, keepdims=False)
    theirs = lax.dynamic_index_in_dim(parts, 1 - core, 1, keepdims=False)
    far, near = (2,), (1, 3, 0)

    def product(side, which):
        rows = jnp.concatenate([side[i] for i in which]) if len(which) > 1 else side[which[0]]
        return jnp.dot(rows, w_out, preferred_element_type=F32)

    far_sent = other_core(product(theirs, far).astype(BF16))
    far_sum = (product(mine, far) + far_sent.astype(F32)).astype(BF16)
    theirs, far_sum = lax.optimization_barrier((theirs, far_sum))
    near_sent = other_core(product(theirs, near).astype(BF16))
    h = width // 2
    from_left = shifted(far_sum[:, :h], "tp", 2)
    from_right = shifted(far_sum[:, h:], "tp", -2)
    near_sum = product(mine, near) + near_sent.astype(F32)
    nxt, prv, own = (near_sum[i * share:(i + 1) * share] for i in range(3))
    a1 = shifted(nxt[:, h:].astype(BF16), "tp", 2)
    b0 = shifted(prv[:, :h].astype(BF16), "tp", -2)
    a0 = shifted((nxt[:, :h] + from_left.astype(F32)).astype(BF16), "tp", 2)
    b1 = shifted((prv[:, h:] + from_right.astype(F32)).astype(BF16), "tp", -2)
    own, a0, a1, b0, b1 = lax.optimization_barrier((own, a0, a1, b0, b1))
    left_half = own[:, :h] + a0.astype(F32) + b0.astype(F32)
    right_half = own[:, h:] + a1.astype(F32) + b1.astype(F32)
    return (gate * jnp.concatenate([left_half, right_half], axis=1)).astype(BF16)


def solution(mesh):
    placed = (
        P(("grp", "sp"), None),
        P(("grp", "sp"), None),
        P("grp"),
        P(),
        P("sp", "tp"),
        P("sp", "tp"),
        P("sp", "tp"),
        P(),
        P(None, "tp"),
        P(None, "tp"),
        P(None, "tp"),
        P(),
        P(),
        P("tp", None),
    )
    return jax.shard_map(
        body, mesh=mesh, in_specs=placed, out_specs=P(("grp", "sp", "tp"), None), check_vma=False
    )
```

```python
import functools

import jax
import jax.numpy as jnp
from jax import lax
from jax.experimental import pallas as pl
from jax.experimental.pallas import tpu as pltpu
from jax.sharding import PartitionSpec as P


HEAD = 128
GRID_W = 64
EPS = 1e-06
CONTEXT_LIFT = 1.5
ROPE_THETA = 10000.0
SCALING = HEAD ** -0.5
LOG2E = 1.4426950408889634


BF16 = jnp.bfloat16
F32 = jnp.float32
VM = pl.BlockSpec(memory_space=pltpu.VMEM)


def rotate_rows(v, cos, sin):
    lane = lax.broadcasted_iota(jnp.int32, v.shape, 1)
    quarter = HEAD // 4
    partner = jnp.where(
        lane % (2 * quarter) < quarter,
        pltpu.roll(v, HEAD - quarter, 1),
        pltpu.roll(v, quarter, 1),
    )
    return v * cos + partner * sin


def rms_head(v, gain):
    return v * lax.rsqrt(jnp.mean(v * v, axis=-1, keepdims=True) + EPS) * gain


def modulation_kernel(lat_hbm, ctx_hbm, scale_hbm, shift_hbm, gate_hbm, out_ref, cond_ref, act_ref, w_ref, sems):
    conds = [
        pltpu.make_async_copy(c, cond_ref.at[i], sems.at[3 + i]) for i, c in enumerate((lat_hbm, ctx_hbm))
    ]
    copies = [
        pltpu.make_async_copy(w, w_ref.at[i], sems.at[i])
        for i, w in enumerate((scale_hbm, shift_hbm, gate_hbm))
    ]
    for c in conds + copies:
        c.start()
    lines = w_ref.shape[1] // 128
    first = lax.axis_index("sp") * lines
    act = []
    for i, c in enumerate(conds):
        c.wait()
        v = cond_ref[i].astype(F32)
        act_ref[i] = v * jax.nn.sigmoid(v)
        act.append(jnp.concatenate([act_ref[i, pl.ds(first + j, 1), :] for j in range(lines)], axis=1))
    act = jnp.concatenate(act, axis=0).astype(BF16)
    pieces = w_ref.shape[2] // 128
    rows, context_rows = [], []
    for i, c in enumerate(copies):
        c.wait()
        part = jnp.dot(act, w_ref[i], preferred_element_type=F32)
        near = part[0:1].astype(BF16).astype(F32)
        rows += [near, part[0:1] - near]
        if i < 2:
            context_rows.append(part[1:2])
    tile = jnp.concatenate(
        [r[:, 128 * j:128 * j + 128] for r in rows + context_rows for j in range(pieces)], axis=0
    ).astype(BF16)
    for i in range(out_ref.shape[0]):
        out_ref[i] = tile


def sum_kernel(in_ref, out_ref):
    total = in_ref[0].astype(F32)
    for i in range(1, in_ref.shape[0]):
        total = total + in_ref[i].astype(F32)
    pieces = in_ref.shape[1] // 8
    for i in range(3):
        at = 2 * i * pieces
        out_ref[i * pieces:(i + 1) * pieces, :] = total[at:at + pieces] + total[at + pieces:at + 2 * pieces]
    out_ref[3 * pieces:5 * pieces, :] = total[6 * pieces:8 * pieces]
    out_ref[5 * pieces:, :] = jnp.zeros((out_ref.shape[0] - 5 * pieces, 128), F32)


def prepare_kernel(x_ref, c_ref, rx_ref, rc_ref):
    tok, width = x_ref.shape
    step = 16

    def rows_of(src, dst, rows):
        total = jnp.zeros((step, 128), F32)
        for j in range(width // 128):
            v = src[rows, 128 * j:128 * j + 128].astype(F32)
            total = total + v * v
        r = lax.rsqrt(jnp.sum(total, axis=-1, keepdims=True) / width + EPS)
        dst[rows, :] = jnp.broadcast_to(r, (step, 128))

    @pl.loop(0, tok // step)
    def _(i):
        rows_of(x_ref, rx_ref, pl.ds(pl.multiple_of(i * step, step), step))

    for i in range(c_ref.shape[0] // step):
        rows_of(c_ref, rc_ref, pl.ds(i * step, step))


def kv_kernel(
    x_ref, c_ref, rx_ref, rc_ref, own_ref, m1_ref, m3_ref, m2_ref, gain_ref, wk_ref, wv_ref, g_ref, cos_ref, sin_ref,
    kv_ref, nm_ref, gate_ref, both_ref, mod_ref, ab_ref, w_ref,
):
    tok, width = x_ref.shape
    ctx = c_ref.shape[0]
    n_tp = lax.axis_size("tp")
    chip, core = lax.axis_index("tp") // 2, lax.axis_index("tp") % 2
    n_x = n_tp // 2
    for back, ref in ((0, own_ref), (1, m1_ref), (3, m3_ref), (2, m2_ref)):
        source = lax.rem(chip + n_x - back, n_x)
        for c in range(2):
            mod_ref[2 * source + lax.rem(core + c, 2)] = ref[c]
    pieces = width // n_tp // 128
    for t in range(n_tp):
        for p in range(pieces):
            cs = slice((t * pieces + p) * 128, (t * pieces + p + 1) * 128)
            piece = [mod_ref[t, i * pieces + p:i * pieces + p + 1, :] for i in range(5)]
            gain = gain_ref[:, cs]
            ab_ref[0:1, cs] = gain * (1.0 + piece[0])
            ab_ref[1:2, cs] = piece[1]
            gate_ref[:, cs] = piece[2]
            ab_ref[2:3, cs] = gain * (1.0 + piece[3])
            ab_ref[3:4, cs] = piece[4]

    step = 64

    @pl.loop(0, tok // step)
    def _(i):
        rows = pl.ds(pl.multiple_of(i * step, step), step)
        r = rx_ref[rows, :]
        for j in range(width // 128):
            cs = slice(128 * j, 128 * j + 128)
            v = x_ref[rows, cs].astype(F32) * r
            nm_ref[rows, cs] = (v * ab_ref[0:1, cs] + ab_ref[1:2, cs]).astype(BF16)

    r = rc_ref[...]
    for j in range(width // 128):
        cs = slice(128 * j, 128 * j + 128)
        nm_ref[tok:tok + ctx, cs] = (c_ref[:, cs].astype(F32) * r * ab_ref[2:3, cs] + ab_ref[3:4, cs]).astype(BF16)

    @pl.loop(0, w_ref.shape[0] // 256)
    def _(i):
        rows = pl.ds(pl.multiple_of(i * 256, 256), 256)
        w_ref[rows, :HEAD] = wk_ref[rows, :]
        w_ref[rows, HEAD:] = wv_ref[rows, :]

    both_ref[...] = jnp.dot(nm_ref[...], w_ref[...], preferred_element_type=F32)
    kv_ref[:, HEAD:] = both_ref[:, HEAD:].astype(BF16)
    gain = g_ref[...]
    tile = 128

    @pl.loop(0, tok // tile)
    def _(i):
        rows = pl.ds(pl.multiple_of(i * tile, tile), tile)
        k = rotate_rows(rms_head(both_ref[rows, :HEAD], gain), cos_ref[rows, :], sin_ref[rows, :])
        kv_ref[rows, :HEAD] = k.astype(BF16)

    kv_ref[tok:tok + ctx, :HEAD] = rms_head(both_ref[tok:tok + ctx, :HEAD], gain).astype(BF16)


def q_kernel(nm_ref, w_ref, g_ref, cos_ref, sin_ref, q_ref, both_ref):
    tok = cos_ref.shape[0]
    heads = w_ref.shape[1] // HEAD
    gain = g_ref[...]
    tile = 128
    both_ref[...] = jnp.dot(nm_ref[:tok, :], w_ref[...], preferred_element_type=F32)

    @pl.loop(0, tok // tile)
    def _(i):
        rows = pl.ds(pl.multiple_of(i * tile, tile), tile)
        for h in range(heads):
            v = rotate_rows(
                rms_head(both_ref[rows, h * HEAD:(h + 1) * HEAD], gain), cos_ref[rows, :], sin_ref[rows, :]
            )
            q_ref[pl.ds(pl.multiple_of(h * tok + i * tile, tile), tile), :] = v.astype(BF16)


def attend_block(q_ref, kv_refs, vt_ref, m_ref, l_ref, acc_ref, cols, tok):
    q = q_ref[cols, :]
    scores = []
    for kv_ref in kv_refs:
        s = lax.dot_general(kv_ref[:, :HEAD], q, (((1,), (1,)), ((), ())), preferred_element_type=F32)
        scores += [s[:tok], s[tok:] + CONTEXT_LIFT / SCALING]
    old = m_ref[0:1, cols]
    new = old
    for s in scores:
        new = jnp.maximum(new, jnp.max(s, axis=0, keepdims=True))
    keep = jnp.exp2((old - new) * (SCALING * LOG2E))
    m_ref[0:1, cols] = new
    total = l_ref[0:1, cols] * keep
    out = acc_ref[:, cols] * keep
    for i in range(len(kv_refs)):
        p = jnp.exp2((jnp.concatenate(scores[2 * i:2 * i + 2], axis=0) - new) * (SCALING * LOG2E))
        total = total + jnp.sum(p, axis=0, keepdims=True)
        out = out + jnp.dot(vt_ref[i], p.astype(BF16), preferred_element_type=F32)
    l_ref[0:1, cols] = total
    acc_ref[:, cols] = out


def attend_kernel(n_kv, first, last, tok, *refs):
    q_ref, kv_refs = refs[0], refs[1:1 + n_kv]
    at = 1 + n_kv
    if not first:
        m_in, l_in, acc_in = refs[at:at + 3]
        at += 3
    if last:
        out_ref = refs[at]
        at += 1
        m_ref, l_ref, acc_ref = refs[at + 1:at + 4]
        vt_ref = refs[at]
    else:
        m_ref, l_ref, acc_ref = refs[at:at + 3]
        vt_ref = refs[at + 3]
    if first:
        m_ref[...] = jnp.full(m_ref.shape, -1e30, F32)
        l_ref[...] = jnp.zeros(l_ref.shape, F32)
        acc_ref[...] = jnp.zeros(acc_ref.shape, F32)
    else:
        m_ref[...] = m_in[...]
        l_ref[...] = l_in[...]
        acc_ref[...] = acc_in[...]
    for i, kv_ref in enumerate(kv_refs):
        vt_ref[i] = jnp.transpose(kv_ref[:, HEAD:])
    queries = q_ref.shape[0]
    width = 256

    @pl.loop(0, queries // width)
    def _(i):
        cols = pl.ds(pl.multiple_of(i * width, width), width)
        attend_block(q_ref, kv_refs, vt_ref, m_ref, l_ref, acc_ref, cols, tok)

    if last:
        for h in range(queries // tok):
            cols = slice(h * tok, (h + 1) * tok)
            done = acc_ref[:, cols] / l_ref[0:1, cols]
            out_ref[:, h * HEAD:(h + 1) * HEAD] = jnp.transpose(done).astype(BF16)


def attend(q, chunks, state, tok, last=False):
    queries = q.shape[0]
    first = state is None
    shapes = [
        jax.ShapeDtypeStruct((8, queries), F32),
        jax.ShapeDtypeStruct((8, queries), F32),
        jax.ShapeDtypeStruct((HEAD, queries), F32),
    ]
    rows = sum(c.shape[0] for c in chunks)
    turned = pltpu.VMEM((len(chunks), HEAD, chunks[0].shape[0]), BF16)
    cost = pl.CostEstimate(
        flops=4 * rows * queries * HEAD, transcendentals=rows * queries, bytes_accessed=1 << 20
    )
    operands = [q, *chunks] + ([] if first else list(state))
    if last:
        return pl.pallas_call(
            functools.partial(attend_kernel, len(chunks), first, True, tok),
            out_shape=jax.ShapeDtypeStruct((tok, queries // tok * HEAD), BF16),
            in_specs=[VM] * len(operands),
            out_specs=VM,
            scratch_shapes=[turned, *[pltpu.VMEM(s.shape, s.dtype) for s in shapes]],
            cost_estimate=cost,
            compiler_params=pltpu.CompilerParams(vmem_limit_bytes=16 << 20),
            name="attend_last",
        )(*operands)
    return pl.pallas_call(
        functools.partial(attend_kernel, len(chunks), first, False, tok),
        out_shape=shapes,
        in_specs=[VM] * len(operands),
        out_specs=[VM] * 3,
        scratch_shapes=[turned],
        input_output_aliases={} if first else {1 + len(chunks) + i: i for i in range(3)},
        cost_estimate=cost,
        compiler_params=pltpu.CompilerParams(vmem_limit_bytes=16 << 20),
        name="attend",
    )(*operands)


def shifted(x, axis, by):
    n = lax.axis_size(axis)
    return lax.ppermute(x, axis, [(i, (i + by) % n) for i in range(n)])


def along_ring(x, by):
    n_sp, n_tp = lax.axis_size("sp"), lax.axis_size("tp")
    pairs = []
    for z in range(n_sp):
        for t in range(n_tp):
            to = (z + (by if t % 2 else -by)) % n_sp
            pairs.append((z * n_tp + t, to * n_tp + t))
    return lax.ppermute(x, ("sp", "tp"), pairs)


def other_core(x):
    n = lax.axis_size("tp")
    return lax.ppermute(x, "tp", [(i, i ^ 1) for i in range(n)])


def body(
    latent, context, cond_latent, cond_context, w_shift, w_scale, w_gate, norm_gain,
    w_query, w_key, w_value, q_gain, k_gain, w_out,
):
    seq_index = lax.axis_index("sp")
    n_sp = lax.axis_size("sp")
    tp_index = lax.axis_index("tp")
    mod_rows, mod_cols = w_shift.shape
    tok, width = latent.shape
    ctx = context.shape[0]

    n_tp = lax.axis_size("tp")
    pieces = mod_cols // 128
    lines = -(-5 * pieces // 8) * 8
    partial_mod = pl.pallas_call(
        modulation_kernel,
        out_shape=jax.ShapeDtypeStruct((n_sp, 8 * pieces, 128), BF16),
        in_specs=[pl.BlockSpec(memory_space=pl.ANY)] * 5,
        out_specs=VM,
        scratch_shapes=[
            pltpu.VMEM((2, width // 128, 128), BF16),
            pltpu.VMEM((2, width // 128, 128), F32),
            pltpu.VMEM((3, mod_rows, mod_cols), BF16),
            pltpu.SemaphoreType.DMA((5,)),
        ],
        compiler_params=pltpu.CompilerParams(vmem_limit_bytes=60 << 20),
        name="modulation",
    )(cond_latent.reshape(-1, 128), cond_context.reshape(-1, 128), w_scale, w_shift, w_gate)
    gathered = lax.all_to_all(partial_mod, "sp", split_axis=0, concat_axis=0, tiled=True)
    rx, rc = pl.pallas_call(
        prepare_kernel,
        out_shape=[
            jax.ShapeDtypeStruct((tok, 128), F32),
            jax.ShapeDtypeStruct((ctx, 128), F32),
        ],
        in_specs=[VM] * 2,
        out_specs=[VM] * 2,
        compiler_params=pltpu.CompilerParams(vmem_limit_bytes=32 << 20),
        cost_estimate=pl.CostEstimate(flops=1 << 30, transcendentals=0, bytes_accessed=12 << 20),
        name="prepare",
    )(latent, context)
    positions = seq_index * tok + jnp.arange(tok, dtype=jnp.int32)
    freqs = HEAD // 4
    inverse = ROPE_THETA ** (-jnp.arange(freqs, dtype=F32) / freqs)
    row = (positions // GRID_W).astype(F32)[:, None] * inverse
    col = (positions % GRID_W).astype(F32)[:, None] * inverse
    cos = jnp.concatenate([jnp.cos(row), jnp.cos(row), jnp.cos(col), jnp.cos(col)], axis=1)
    sin = jnp.concatenate([-jnp.sin(row), jnp.sin(row), -jnp.sin(col), jnp.sin(col)], axis=1)

    gathered, rx, rc, cos, sin = lax.optimization_barrier((gathered, rx, rc, cos, sin))
    summed = pl.pallas_call(
        sum_kernel,
        out_shape=jax.ShapeDtypeStruct((lines, 128), F32),
        in_specs=[VM],
        out_specs=VM,
        compiler_params=pltpu.CompilerParams(vmem_limit_bytes=8 << 20),
        cost_estimate=pl.CostEstimate(flops=8 << 30, transcendentals=0, bytes_accessed=1 << 20),
        name="sum_parts",
    )(gathered)
    pair = jnp.stack([summed, other_core(summed)])
    columns = [pair, shifted(pair, "tp", 2), shifted(pair, "tp", -2), shifted(pair, "tp", 4)]

    kv, normed, gate = pl.pallas_call(
        kv_kernel,
        out_shape=[
            jax.ShapeDtypeStruct((tok + ctx, 2 * HEAD), BF16),
            jax.ShapeDtypeStruct((tok + ctx, width), BF16),
            jax.ShapeDtypeStruct((1, width), F32),
        ],
        in_specs=[VM] * 14,
        out_specs=[VM] * 3,
        scratch_shapes=[
            pltpu.VMEM((tok + ctx, 2 * HEAD), F32),
            pltpu.VMEM((n_tp, lines, 128), F32),
            pltpu.VMEM((8, width), F32),
            pltpu.VMEM((width, 2 * HEAD), BF16),
        ],
        cost_estimate=pl.CostEstimate(flops=2 * tok * width * 256, transcendentals=0, bytes_accessed=1 << 22),
        compiler_params=pltpu.CompilerParams(vmem_limit_bytes=24 << 20),
        name="project_kv",
    )(
        latent, context, rx, rc, *columns, norm_gain.reshape(1, width), w_key, w_value, k_gain.reshape(1, HEAD),
        cos, sin,
    )

    right, left = along_ring(kv, 1), along_ring(kv, -1)
    q = pl.pallas_call(
        q_kernel,
        out_shape=jax.ShapeDtypeStruct((w_query.shape[1] // HEAD * tok, HEAD), BF16),
        in_specs=[VM] * 5,
        out_specs=VM,
        scratch_shapes=[pltpu.VMEM((tok, w_query.shape[1]), F32)],
        cost_estimate=pl.CostEstimate(flops=2 * tok * width * 256, transcendentals=0, bytes_accessed=1 << 22),
        compiler_params=pltpu.CompilerParams(vmem_limit_bytes=24 << 20),
        name="project_q",
    )(normed, w_query, q_gain.reshape(1, HEAD), cos, sin)
    state = attend(q, [kv], None, tok)
    half = n_sp // 2
    for step in range(1, half):
        right, m = lax.optimization_barrier((right, state[0]))
        left, m = lax.optimization_barrier((left, m))
        state = [m, *state[1:]]
        now = [right, left]
        right = along_ring(right, 1)
        if step + 1 < half:
            left = along_ring(left, -1)
        state = attend(q, now, state, tok)
    attended = attend(q, [right], state, tok, last=True)

    n_x = lax.axis_size("tp") // 2
    core, chip = tp_index % 2, tp_index // 2
    share = tok // (2 * n_x)
    parts = attended.reshape(n_x, 2, share, attended.shape[1])
    parts = jnp.concatenate([parts, parts], axis=0)
    parts = lax.dynamic_slice_in_dim(parts, chip, n_x, 0)
    mine = lax.dynamic_index_in_dim(parts, core, 1, keepdims=False)
    theirs = lax.dynamic_index_in_dim(parts, 1 - core, 1, keepdims=False)
    far, near = (2,), (1, 3, 0)

    def product(side, which):
        rows = jnp.concatenate([side[i] for i in which]) if len(which) > 1 else side[which[0]]
        return jnp.dot(rows, w_out, preferred_element_type=F32)

    far_sent = other_core(product(theirs, far).astype(BF16))
    far_sum = (product(mine, far) + far_sent.astype(F32)).astype(BF16)
    theirs, far_sum = lax.optimization_barrier((theirs, far_sum))
    near_sent = other_core(product(theirs, near).astype(BF16))
    h = width // 2
    from_left = shifted(far_sum[:, :h], "tp", 2)
    from_right = shifted(far_sum[:, h:], "tp", -2)
    near_sum = product(mine, near) + near_sent.astype(F32)
    nxt, prv, own = (near_sum[i * share:(i + 1) * share] for i in range(3))
    halves = (nxt[:, h:].astype(BF16), prv[:, :h].astype(BF16))
    a1 = shifted(halves[0], "tp", 2)
    b0 = shifted(halves[1], "tp", -2)
    joined = ((nxt[:, :h] + from_left.astype(F32)).astype(BF16), (prv[:, h:] + from_right.astype(F32)).astype(BF16))
    a0 = shifted(joined[0], "tp", 2)
    b1 = shifted(joined[1], "tp", -2)
    own, a0, a1, b0, b1 = lax.optimization_barrier((own, a0, a1, b0, b1))
    left_half = own[:, :h] + a0.astype(F32) + b0.astype(F32)
    right_half = own[:, h:] + a1.astype(F32) + b1.astype(F32)
    return (gate * jnp.concatenate([left_half, right_half], axis=1)).astype(BF16)


def solution(mesh):
    placed = (
        P(("grp", "sp"), None),
        P(("grp", "sp"), None),
        P("grp"),
        P(),
        P("sp", "tp"),
        P("sp", "tp"),
        P("sp", "tp"),
        P(),
        P(None, "tp"),
        P(None, "tp"),
        P(None, "tp"),
        P(),
        P(),
        P("tp", None),
    )
    return jax.shard_map(
        body, mesh=mesh, in_specs=placed, out_specs=P(("grp", "sp", "tp"), None), check_vma=False
    )
```

```python
import functools

import jax
import jax.numpy as jnp
from jax import lax
from jax.experimental import pallas as pl
from jax.experimental.pallas import tpu as pltpu
from jax.sharding import PartitionSpec as P


HEAD = 128
GRID_W = 64
EPS = 1e-06
CONTEXT_LIFT = 1.5
ROPE_THETA = 10000.0
SCALING = HEAD ** -0.5
LOG2E = 1.4426950408889634


BF16 = jnp.bfloat16
F32 = jnp.float32
VM = pl.BlockSpec(memory_space=pltpu.VMEM)


def rotate_rows(v, cos, sin):
    lane = lax.broadcasted_iota(jnp.int32, v.shape, 1)
    quarter = HEAD // 4
    partner = jnp.where(
        lane % (2 * quarter) < quarter,
        pltpu.roll(v, HEAD - quarter, 1),
        pltpu.roll(v, quarter, 1),
    )
    return v * cos + partner * sin


def rms_head(v, gain):
    return v * lax.rsqrt(jnp.mean(v * v, axis=-1, keepdims=True) + EPS) * gain


def modulation_kernel(lat_hbm, ctx_hbm, scale_hbm, shift_hbm, gate_hbm, out_ref, cond_ref, act_ref, w_ref, sems):
    conds = [
        pltpu.make_async_copy(c, cond_ref.at[i], sems.at[3 + i]) for i, c in enumerate((lat_hbm, ctx_hbm))
    ]
    copies = [
        pltpu.make_async_copy(w, w_ref.at[i], sems.at[i])
        for i, w in enumerate((scale_hbm, shift_hbm, gate_hbm))
    ]
    for c in conds + copies:
        c.start()
    lines = w_ref.shape[1] // 128
    first = lax.axis_index("sp") * lines
    act = []
    for i, c in enumerate(conds):
        c.wait()
        v = cond_ref[i].astype(F32)
        act_ref[i] = v * jax.nn.sigmoid(v)
        act.append(jnp.concatenate([act_ref[i, pl.ds(first + j, 1), :] for j in range(lines)], axis=1))
    act = jnp.concatenate(act, axis=0).astype(BF16)
    pieces = w_ref.shape[2] // 128
    rows, context_rows = [], []
    for i, c in enumerate(copies):
        c.wait()
        part = jnp.dot(act, w_ref[i], preferred_element_type=F32)
        near = part[0:1].astype(BF16).astype(F32)
        rows += [near, part[0:1] - near]
        if i < 2:
            context_rows.append(part[1:2])
    tile = jnp.concatenate(
        [r[:, 128 * j:128 * j + 128] for r in rows + context_rows for j in range(pieces)], axis=0
    ).astype(BF16)
    for i in range(out_ref.shape[0]):
        out_ref[i] = tile


def sum_kernel(in_ref, out_ref):
    total = in_ref[0].astype(F32)
    for i in range(1, in_ref.shape[0]):
        total = total + in_ref[i].astype(F32)
    pieces = in_ref.shape[1] // 8
    for i in range(3):
        at = 2 * i * pieces
        out_ref[i * pieces:(i + 1) * pieces, :] = total[at:at + pieces] + total[at + pieces:at + 2 * pieces]
    out_ref[3 * pieces:5 * pieces, :] = total[6 * pieces:8 * pieces]
    out_ref[5 * pieces:, :] = jnp.zeros((out_ref.shape[0] - 5 * pieces, 128), F32)


def prepare_kernel(x_ref, c_ref, wk_ref, wv_ref, rx_ref, rc_ref, w_ref):
    tok, width = x_ref.shape
    step = 16

    def rows_of(src, dst, rows):
        total = jnp.zeros((step, 128), F32)
        for j in range(width // 128):
            v = src[rows, 128 * j:128 * j + 128].astype(F32)
            total = total + v * v
        r = lax.rsqrt(jnp.sum(total, axis=-1, keepdims=True) / width + EPS)
        dst[rows, :] = jnp.broadcast_to(r, (step, 128))

    @pl.loop(0, tok // step)
    def _(i):
        rows_of(x_ref, rx_ref, pl.ds(pl.multiple_of(i * step, step), step))

    for i in range(c_ref.shape[0] // step):
        rows_of(c_ref, rc_ref, pl.ds(i * step, step))

    @pl.loop(0, w_ref.shape[0] // 256)
    def _(i):
        rows = pl.ds(pl.multiple_of(i * 256, 256), 256)
        w_ref[rows, :HEAD] = wk_ref[rows, :]
        w_ref[rows, HEAD:] = wv_ref[rows, :]


def kv_kernel(
    x_ref, c_ref, rx_ref, rc_ref, own_ref, m1_ref, m3_ref, m2_ref, gain_ref, w_ref, g_ref, cos_ref, sin_ref,
    kv_ref, nm_ref, gate_ref, both_ref, mod_ref, ab_ref,
):
    tok, width = x_ref.shape
    ctx = c_ref.shape[0]
    n_tp = lax.axis_size("tp")
    chip, core = lax.axis_index("tp") // 2, lax.axis_index("tp") % 2
    n_x = n_tp // 2
    for back, ref in ((0, own_ref), (1, m1_ref), (3, m3_ref), (2, m2_ref)):
        source = lax.rem(chip + n_x - back, n_x)
        for c in range(2):
            mod_ref[2 * source + lax.rem(core + c, 2)] = ref[c]
    pieces = width // n_tp // 128
    for t in range(n_tp):
        for p in range(pieces):
            cs = slice((t * pieces + p) * 128, (t * pieces + p + 1) * 128)
            piece = [mod_ref[t, i * pieces + p:i * pieces + p + 1, :] for i in range(5)]
            gain = gain_ref[:, cs]
            ab_ref[0:1, cs] = gain * (1.0 + piece[0])
            ab_ref[1:2, cs] = piece[1]
            gate_ref[:, cs] = piece[2]
            ab_ref[2:3, cs] = gain * (1.0 + piece[3])
            ab_ref[3:4, cs] = piece[4]

    chunk, step = width // 4, 64
    both = None
    for k in range(0, width, chunk):
        for j in range(k, k + chunk, 128):
            cs = slice(j, j + 128)
            for i in range(0, tok, step):
                rows = slice(i, i + step)
                v = x_ref[rows, cs].astype(F32) * rx_ref[rows, :]
                nm_ref[rows, cs] = (v * ab_ref[0:1, cs] + ab_ref[1:2, cs]).astype(BF16)
            v = c_ref[:, cs].astype(F32) * rc_ref[...]
            nm_ref[tok:tok + ctx, cs] = (v * ab_ref[2:3, cs] + ab_ref[3:4, cs]).astype(BF16)
        part = jnp.dot(nm_ref[:, k:k + chunk], w_ref[k:k + chunk, :], preferred_element_type=F32)
        both = part if both is None else both + part
    both_ref[...] = both
    kv_ref[:, HEAD:] = both_ref[:, HEAD:].astype(BF16)
    gain = g_ref[...]
    tile = 128

    @pl.loop(0, tok // tile)
    def _(i):
        rows = pl.ds(pl.multiple_of(i * tile, tile), tile)
        k = rotate_rows(rms_head(both_ref[rows, :HEAD], gain), cos_ref[rows, :], sin_ref[rows, :])
        kv_ref[rows, :HEAD] = k.astype(BF16)

    kv_ref[tok:tok + ctx, :HEAD] = rms_head(both_ref[tok:tok + ctx, :HEAD], gain).astype(BF16)


def q_kernel(nm_ref, w_ref, g_ref, cos_ref, sin_ref, q_ref, both_ref):
    tok = cos_ref.shape[0]
    heads = w_ref.shape[1] // HEAD
    gain = g_ref[...]
    tile = 128
    both_ref[...] = jnp.dot(nm_ref[:tok, :], w_ref[...], preferred_element_type=F32)

    @pl.loop(0, tok // tile)
    def _(i):
        rows = pl.ds(pl.multiple_of(i * tile, tile), tile)
        for h in range(heads):
            v = rotate_rows(
                rms_head(both_ref[rows, h * HEAD:(h + 1) * HEAD], gain), cos_ref[rows, :], sin_ref[rows, :]
            )
            q_ref[pl.ds(pl.multiple_of(h * tok + i * tile, tile), tile), :] = v.astype(BF16)


def attend_block(q_ref, kv_refs, vt_refs, m_ref, l_ref, acc_ref, cols, latents):
    q = q_ref[cols, :]
    scores = []
    for kv_ref, lat in zip(kv_refs, latents, strict=True):
        s = lax.dot_general(kv_ref[:, :HEAD], q, (((1,), (1,)), ((), ())), preferred_element_type=F32)
        if lat < kv_ref.shape[0]:
            s = jnp.concatenate([s[:lat], s[lat:] + CONTEXT_LIFT / SCALING], axis=0)
        scores.append(s)
    old = m_ref[0:1, cols]
    new = old
    for s in scores:
        new = jnp.maximum(new, jnp.max(s, axis=0, keepdims=True))
    keep = jnp.exp2((old - new) * (SCALING * LOG2E))
    m_ref[0:1, cols] = new
    total = l_ref[0:1, cols] * keep
    out = acc_ref[:, cols] * keep
    for s, vt_ref in zip(scores, vt_refs, strict=True):
        p = jnp.exp2((s - new) * (SCALING * LOG2E))
        total = total + jnp.sum(p, axis=0, keepdims=True)
        out = out + jnp.dot(vt_ref[...], p.astype(BF16), preferred_element_type=F32)
    l_ref[0:1, cols] = total
    acc_ref[:, cols] = out


def attend_kernel(latents, first, last, tok, *refs):
    n_kv = len(latents)
    q_ref, kv_refs = refs[0], refs[1:1 + n_kv]
    at = 1 + n_kv
    if not first:
        m_in, l_in, acc_in = refs[at:at + 3]
        at += 3
    if last:
        out_ref = refs[at]
        at += 1
    m_ref, l_ref, acc_ref = refs[at:at + 3]
    vt_refs = refs[at + 3:]
    if first:
        m_ref[...] = jnp.full(m_ref.shape, -1e30, F32)
        l_ref[...] = jnp.zeros(l_ref.shape, F32)
        acc_ref[...] = jnp.zeros(acc_ref.shape, F32)
    else:
        m_ref[...] = m_in[...]
        l_ref[...] = l_in[...]
        acc_ref[...] = acc_in[...]
    for kv_ref, vt_ref in zip(kv_refs, vt_refs, strict=True):
        vt_ref[...] = jnp.transpose(kv_ref[:, HEAD:])
    queries = q_ref.shape[0]
    width = 256
    if last:
        for i in range(0, queries, width):
            attend_block(q_ref, kv_refs, vt_refs, m_ref, l_ref, acc_ref, slice(i, i + width), latents)
        for h in range(queries // tok):
            cols = slice(h * tok, (h + 1) * tok)
            done = acc_ref[:, cols] / l_ref[0:1, cols]
            out_ref[:, h * HEAD:(h + 1) * HEAD] = jnp.transpose(done).astype(BF16)
    else:

        @pl.loop(0, queries // width)
        def _(i):
            cols = pl.ds(pl.multiple_of(i * width, width), width)
            attend_block(q_ref, kv_refs, vt_refs, m_ref, l_ref, acc_ref, cols, latents)


def attend(q, chunks, state, tok, latents=None, last=False):
    queries = q.shape[0]
    first = state is None
    latents = latents or [tok] * len(chunks)
    shapes = [
        jax.ShapeDtypeStruct((8, queries), F32),
        jax.ShapeDtypeStruct((8, queries), F32),
        jax.ShapeDtypeStruct((HEAD, queries), F32),
    ]
    rows = sum(c.shape[0] for c in chunks)
    turned = [pltpu.VMEM((HEAD, c.shape[0]), BF16) for c in chunks]
    cost = pl.CostEstimate(
        flops=4 * rows * queries * HEAD, transcendentals=rows * queries, bytes_accessed=1 << 20
    )
    operands = [q, *chunks] + ([] if first else list(state))
    kernel = functools.partial(attend_kernel, latents, first, last, tok)
    if last:
        return pl.pallas_call(
            kernel,
            out_shape=jax.ShapeDtypeStruct((tok, queries // tok * HEAD), BF16),
            in_specs=[VM] * len(operands),
            out_specs=VM,
            scratch_shapes=[*[pltpu.VMEM(s.shape, s.dtype) for s in shapes], *turned],
            cost_estimate=cost,
            compiler_params=pltpu.CompilerParams(vmem_limit_bytes=16 << 20),
            name="attend_last",
        )(*operands)
    return pl.pallas_call(
        kernel,
        out_shape=shapes,
        in_specs=[VM] * len(operands),
        out_specs=[VM] * 3,
        scratch_shapes=turned,
        input_output_aliases={} if first else {1 + len(chunks) + i: i for i in range(3)},
        cost_estimate=cost,
        compiler_params=pltpu.CompilerParams(vmem_limit_bytes=16 << 20),
        name="attend",
    )(*operands)


def shifted(x, axis, by):
    n = lax.axis_size(axis)
    return lax.ppermute(x, axis, [(i, (i + by) % n) for i in range(n)])


def along_ring(x, by):
    n_sp, n_tp = lax.axis_size("sp"), lax.axis_size("tp")
    pairs = []
    for z in range(n_sp):
        for t in range(n_tp):
            to = (z + (by if t % 2 else -by)) % n_sp
            pairs.append((z * n_tp + t, to * n_tp + t))
    return lax.ppermute(x, ("sp", "tp"), pairs)


def other_core(x):
    n = lax.axis_size("tp")
    return lax.ppermute(x, "tp", [(i, i ^ 1) for i in range(n)])


def body(
    latent, context, cond_latent, cond_context, w_shift, w_scale, w_gate, norm_gain,
    w_query, w_key, w_value, q_gain, k_gain, w_out,
):
    seq_index = lax.axis_index("sp")
    n_sp = lax.axis_size("sp")
    tp_index = lax.axis_index("tp")
    mod_rows, mod_cols = w_shift.shape
    tok, width = latent.shape
    ctx = context.shape[0]

    n_tp = lax.axis_size("tp")
    pieces = mod_cols // 128
    lines = -(-5 * pieces // 8) * 8
    partial_mod = pl.pallas_call(
        modulation_kernel,
        out_shape=jax.ShapeDtypeStruct((n_sp, 8 * pieces, 128), BF16),
        in_specs=[pl.BlockSpec(memory_space=pl.ANY)] * 5,
        out_specs=VM,
        scratch_shapes=[
            pltpu.VMEM((2, width // 128, 128), BF16),
            pltpu.VMEM((2, width // 128, 128), F32),
            pltpu.VMEM((3, mod_rows, mod_cols), BF16),
            pltpu.SemaphoreType.DMA((5,)),
        ],
        compiler_params=pltpu.CompilerParams(vmem_limit_bytes=60 << 20),
        name="modulation",
    )(cond_latent.reshape(-1, 128), cond_context.reshape(-1, 128), w_scale, w_shift, w_gate)
    gathered = lax.all_to_all(partial_mod, "sp", split_axis=0, concat_axis=0, tiled=True)
    rx, rc, w_kv = pl.pallas_call(
        prepare_kernel,
        out_shape=[
            jax.ShapeDtypeStruct((tok, 128), F32),
            jax.ShapeDtypeStruct((ctx, 128), F32),
            jax.ShapeDtypeStruct((width, 2 * HEAD), BF16),
        ],
        in_specs=[VM] * 4,
        out_specs=[VM] * 3,
        compiler_params=pltpu.CompilerParams(vmem_limit_bytes=32 << 20),
        cost_estimate=pl.CostEstimate(flops=1 << 30, transcendentals=0, bytes_accessed=12 << 20),
        name="prepare",
    )(latent, context, w_key, w_value)
    positions = seq_index * tok + jnp.arange(tok, dtype=jnp.int32)
    freqs = HEAD // 4
    inverse = ROPE_THETA ** (-jnp.arange(freqs, dtype=F32) / freqs)
    row = (positions // GRID_W).astype(F32)[:, None] * inverse
    col = (positions % GRID_W).astype(F32)[:, None] * inverse
    cos = jnp.concatenate([jnp.cos(row), jnp.cos(row), jnp.cos(col), jnp.cos(col)], axis=1)
    sin = jnp.concatenate([-jnp.sin(row), jnp.sin(row), -jnp.sin(col), jnp.sin(col)], axis=1)

    gathered, rx, rc, w_kv, cos, sin = lax.optimization_barrier((gathered, rx, rc, w_kv, cos, sin))
    summed = pl.pallas_call(
        sum_kernel,
        out_shape=jax.ShapeDtypeStruct((lines, 128), F32),
        in_specs=[VM],
        out_specs=VM,
        compiler_params=pltpu.CompilerParams(vmem_limit_bytes=8 << 20),
        cost_estimate=pl.CostEstimate(flops=8 << 30, transcendentals=0, bytes_accessed=1 << 20),
        name="sum_parts",
    )(gathered)
    pair = jnp.stack([summed, other_core(summed)])
    columns = [pair, shifted(pair, "tp", 2), shifted(pair, "tp", -2)]
    columns.append(shifted(pair, "tp", 4))

    kv, normed, gate = pl.pallas_call(
        kv_kernel,
        out_shape=[
            jax.ShapeDtypeStruct((tok + ctx, 2 * HEAD), BF16),
            jax.ShapeDtypeStruct((tok + ctx, width), BF16),
            jax.ShapeDtypeStruct((1, width), F32),
        ],
        in_specs=[VM] * 13,
        out_specs=[VM] * 3,
        scratch_shapes=[
            pltpu.VMEM((tok + ctx, 2 * HEAD), F32),
            pltpu.VMEM((n_tp, lines, 128), F32),
            pltpu.VMEM((8, width), F32),
        ],
        cost_estimate=pl.CostEstimate(flops=2 * tok * width * 256, transcendentals=0, bytes_accessed=1 << 22),
        compiler_params=pltpu.CompilerParams(vmem_limit_bytes=24 << 20),
        name="project_kv",
    )(
        latent, context, rx, rc, *columns, norm_gain.reshape(1, width), w_kv, k_gain.reshape(1, HEAD), cos, sin
    )

    right, left = along_ring(kv, 1), along_ring(kv, -1)
    q = pl.pallas_call(
        q_kernel,
        out_shape=jax.ShapeDtypeStruct((w_query.shape[1] // HEAD * tok, HEAD), BF16),
        in_specs=[VM] * 5,
        out_specs=VM,
        scratch_shapes=[pltpu.VMEM((tok, w_query.shape[1]), F32)],
        cost_estimate=pl.CostEstimate(flops=2 * tok * width * 256, transcendentals=0, bytes_accessed=1 << 22),
        compiler_params=pltpu.CompilerParams(vmem_limit_bytes=24 << 20),
        name="project_q",
    )(normed, w_query, q_gain.reshape(1, HEAD), cos, sin)
    state = attend(q, [kv], None, tok)
    half = n_sp // 2
    cut = (tok + ctx) // 32 * 16
    for step in range(1, half):
        right, m = lax.optimization_barrier((right, state[0]))
        left, m = lax.optimization_barrier((left, m))
        state = [m, *state[1:]]
        now = [right, left]
        if step + 1 == half:
            right, left = right[:cut], left[cut:]
        right = along_ring(right, 1)
        left = along_ring(left, -1)
        state = attend(q, now, state, tok)
    attended = attend(q, [right, left], state, tok, [cut, tok - cut], last=True)

    n_x = lax.axis_size("tp") // 2
    core, chip = tp_index % 2, tp_index // 2
    share = tok // (2 * n_x)
    parts = attended.reshape(n_x, 2, share, attended.shape[1])
    parts = jnp.concatenate([parts, parts], axis=0)
    parts = lax.dynamic_slice_in_dim(parts, chip, n_x, 0)
    mine = lax.dynamic_index_in_dim(parts, core, 1, keepdims=False)
    theirs = lax.dynamic_index_in_dim(parts, 1 - core, 1, keepdims=False)
    far, near = (2,), (1, 3, 0)

    def product(side, which):
        rows = jnp.concatenate([side[i] for i in which]) if len(which) > 1 else side[which[0]]
        return jnp.dot(rows, w_out, preferred_element_type=F32)

    far_sent = other_core(product(theirs, far).astype(BF16))
    own_far, own_near, their_near = lax.optimization_barrier(
        (product(mine, far), product(mine, near), product(theirs, near).astype(BF16))
    )
    far_sum = (own_far + far_sent.astype(F32)).astype(BF16)
    their_near, far_sum = lax.optimization_barrier((their_near, far_sum))
    near_sent = other_core(their_near)
    h = width // 2
    from_left = shifted(far_sum[:, :h], "tp", 2)
    from_right = shifted(far_sum[:, h:], "tp", -2)
    near_sum = own_near + near_sent.astype(F32)
    nxt, prv, own = (near_sum[i * share:(i + 1) * share] for i in range(3))
    halves = (nxt[:, h:].astype(BF16), prv[:, :h].astype(BF16))
    a1 = shifted(halves[0], "tp", 2)
    b0 = shifted(halves[1], "tp", -2)
    joined = ((nxt[:, :h] + from_left.astype(F32)).astype(BF16), (prv[:, h:] + from_right.astype(F32)).astype(BF16))
    a0 = shifted(joined[0], "tp", 2)
    b1 = shifted(joined[1], "tp", -2)
    own, a0, a1, b0, b1 = lax.optimization_barrier((own, a0, a1, b0, b1))
    left_half = own[:, :h] + a0.astype(F32) + b0.astype(F32)
    right_half = own[:, h:] + a1.astype(F32) + b1.astype(F32)
    return (gate * jnp.concatenate([left_half, right_half], axis=1)).astype(BF16)


def solution(mesh):
    placed = (
        P(("grp", "sp"), None),
        P(("grp", "sp"), None),
        P("grp"),
        P(),
        P("sp", "tp"),
        P("sp", "tp"),
        P("sp", "tp"),
        P(),
        P(None, "tp"),
        P(None, "tp"),
        P(None, "tp"),
        P(),
        P(),
        P("tp", None),
    )
    return jax.shard_map(
        body, mesh=mesh, in_specs=placed, out_specs=P(("grp", "sp", "tp"), None), check_vma=False
    )
```

```python
import functools

import jax
import jax.numpy as jnp
from jax import lax
from jax.experimental import pallas as pl
from jax.experimental.pallas import tpu as pltpu
from jax.sharding import PartitionSpec as P


HEAD = 128
GRID_W = 64
EPS = 1e-06
CONTEXT_LIFT = 1.5
ROPE_THETA = 10000.0
SCALING = HEAD ** -0.5
LOG2E = 1.4426950408889634


BF16 = jnp.bfloat16
F32 = jnp.float32
VM = pl.BlockSpec(memory_space=pltpu.VMEM)


def rotate_rows(v, cos, sin):
    lane = lax.broadcasted_iota(jnp.int32, v.shape, 1)
    quarter = HEAD // 4
    partner = jnp.where(
        lane % (2 * quarter) < quarter,
        pltpu.roll(v, HEAD - quarter, 1),
        pltpu.roll(v, quarter, 1),
    )
    return v * cos + partner * sin


def rms_head(v, gain):
    return v * lax.rsqrt(jnp.mean(v * v, axis=-1, keepdims=True) + EPS) * gain


def modulation_kernel(lat_hbm, ctx_hbm, scale_hbm, shift_hbm, gate_hbm, out_ref, cond_ref, act_ref, w_ref, sems):
    conds = [
        pltpu.make_async_copy(c, cond_ref.at[i], sems.at[3 + i]) for i, c in enumerate((lat_hbm, ctx_hbm))
    ]
    copies = [
        pltpu.make_async_copy(w, w_ref.at[i], sems.at[i])
        for i, w in enumerate((scale_hbm, shift_hbm, gate_hbm))
    ]
    for c in conds + copies:
        c.start()
    lines = w_ref.shape[1] // 128
    first = lax.axis_index("sp") * lines
    act = []
    for i, c in enumerate(conds):
        c.wait()
        v = cond_ref[i].astype(F32)
        act_ref[i] = v * jax.nn.sigmoid(v)
        act.append(jnp.concatenate([act_ref[i, pl.ds(first + j, 1), :] for j in range(lines)], axis=1))
    act = jnp.concatenate(act, axis=0).astype(BF16)
    pieces = w_ref.shape[2] // 128
    rows, context_rows = [], []
    for i, c in enumerate(copies):
        c.wait()
        part = jnp.dot(act, w_ref[i], preferred_element_type=F32)
        near = part[0:1].astype(BF16).astype(F32)
        rows += [near, part[0:1] - near]
        if i < 2:
            context_rows.append(part[1:2])
    tile = jnp.concatenate(
        [r[:, 128 * j:128 * j + 128] for r in rows + context_rows for j in range(pieces)], axis=0
    ).astype(BF16)
    for i in range(out_ref.shape[0]):
        out_ref[i] = tile


def sum_kernel(in_ref, out_ref):
    total = in_ref[0].astype(F32)
    for i in range(1, in_ref.shape[0]):
        total = total + in_ref[i].astype(F32)
    pieces = in_ref.shape[1] // 8
    for i in range(3):
        at = 2 * i * pieces
        out_ref[i * pieces:(i + 1) * pieces, :] = total[at:at + pieces] + total[at + pieces:at + 2 * pieces]
    out_ref[3 * pieces:5 * pieces, :] = total[6 * pieces:8 * pieces]
    out_ref[5 * pieces:, :] = jnp.zeros((out_ref.shape[0] - 5 * pieces, 128), F32)


def prepare_kernel(x_ref, c_ref, wk_ref, wv_ref, rx_ref, rc_ref, w_ref):
    tok, width = x_ref.shape
    step = 16

    def rows_of(src, dst, rows):
        total = jnp.zeros((step, 128), F32)
        for j in range(width // 128):
            v = src[rows, 128 * j:128 * j + 128].astype(F32)
            total = total + v * v
        r = lax.rsqrt(jnp.sum(total, axis=-1, keepdims=True) / width + EPS)
        dst[rows, :] = jnp.broadcast_to(r, (step, 128))

    @pl.loop(0, tok // step)
    def _(i):
        rows_of(x_ref, rx_ref, pl.ds(pl.multiple_of(i * step, step), step))

    for i in range(c_ref.shape[0] // step):
        rows_of(c_ref, rc_ref, pl.ds(i * step, step))

    @pl.loop(0, w_ref.shape[0] // 256)
    def _(i):
        rows = pl.ds(pl.multiple_of(i * 256, 256), 256)
        w_ref[rows, :HEAD] = wk_ref[rows, :]
        w_ref[rows, HEAD:] = wv_ref[rows, :]


def kv_kernel(
    x_ref, c_ref, rx_ref, rc_ref, own_ref, m1_ref, m3_ref, m2_ref, gain_ref, w_ref, g_ref, cos_ref, sin_ref,
    kv_ref, nm_ref, gate_ref, both_ref, mod_ref, ab_ref,
):
    tok, width = x_ref.shape
    ctx = c_ref.shape[0]
    n_tp = lax.axis_size("tp")
    chip, core = lax.axis_index("tp") // 2, lax.axis_index("tp") % 2
    n_x = n_tp // 2
    for back, ref in ((0, own_ref), (1, m1_ref), (3, m3_ref), (2, m2_ref)):
        source = lax.rem(chip + n_x - back, n_x)
        for c in range(2):
            mod_ref[2 * source + lax.rem(core + c, 2)] = ref[c]
    pieces = width // n_tp // 128
    for t in range(n_tp):
        for p in range(pieces):
            cs = slice((t * pieces + p) * 128, (t * pieces + p + 1) * 128)
            piece = [mod_ref[t, i * pieces + p:i * pieces + p + 1, :] for i in range(5)]
            gain = gain_ref[:, cs]
            ab_ref[0:1, cs] = gain * (1.0 + piece[0])
            ab_ref[1:2, cs] = piece[1]
            gate_ref[:, cs] = piece[2]
            ab_ref[2:3, cs] = gain * (1.0 + piece[3])
            ab_ref[3:4, cs] = piece[4]

    chunk, step = width // 4, 64
    both = None
    for k in range(0, width, chunk):
        for j in range(k, k + chunk, 128):
            cs = slice(j, j + 128)
            for i in range(0, tok, step):
                rows = slice(i, i + step)
                v = x_ref[rows, cs].astype(F32) * rx_ref[rows, :]
                nm_ref[rows, cs] = (v * ab_ref[0:1, cs] + ab_ref[1:2, cs]).astype(BF16)
            v = c_ref[:, cs].astype(F32) * rc_ref[...]
            nm_ref[tok:tok + ctx, cs] = (v * ab_ref[2:3, cs] + ab_ref[3:4, cs]).astype(BF16)
        part = jnp.dot(nm_ref[:, k:k + chunk], w_ref[k:k + chunk, :], preferred_element_type=F32)
        both = part if both is None else both + part
    both_ref[...] = both
    kv_ref[:, HEAD:] = both_ref[:, HEAD:].astype(BF16)
    gain = g_ref[...]
    tile = 128

    @pl.loop(0, tok // tile)
    def _(i):
        rows = pl.ds(pl.multiple_of(i * tile, tile), tile)
        k = rotate_rows(rms_head(both_ref[rows, :HEAD], gain), cos_ref[rows, :], sin_ref[rows, :])
        kv_ref[rows, :HEAD] = k.astype(BF16)

    kv_ref[tok:tok + ctx, :HEAD] = rms_head(both_ref[tok:tok + ctx, :HEAD], gain).astype(BF16)


def q_kernel(nm_ref, w_ref, g_ref, cos_ref, sin_ref, q_ref, both_ref):
    tok = cos_ref.shape[0]
    heads = w_ref.shape[1] // HEAD
    gain = g_ref[...]
    tile = 128
    both_ref[...] = jnp.dot(nm_ref[:tok, :], w_ref[...], preferred_element_type=F32)

    @pl.loop(0, tok // tile)
    def _(i):
        rows = pl.ds(pl.multiple_of(i * tile, tile), tile)
        for h in range(heads):
            v = rotate_rows(
                rms_head(both_ref[rows, h * HEAD:(h + 1) * HEAD], gain), cos_ref[rows, :], sin_ref[rows, :]
            )
            q_ref[pl.ds(pl.multiple_of(h * tok + i * tile, tile), tile), :] = v.astype(BF16)


def attend_block(q_ref, kv_refs, vt_refs, m_ref, l_ref, acc_ref, cols, latents):
    q = q_ref[cols, :]
    scores = []
    for kv_ref, lat in zip(kv_refs, latents, strict=True):
        s = lax.dot_general(kv_ref[:, :HEAD], q, (((1,), (1,)), ((), ())), preferred_element_type=F32)
        if lat < kv_ref.shape[0]:
            s = jnp.concatenate([s[:lat], s[lat:] + CONTEXT_LIFT / SCALING], axis=0)
        scores.append(s)
    old = m_ref[0:1, cols]
    new = old
    for s in scores:
        new = jnp.maximum(new, jnp.max(s, axis=0, keepdims=True))
    keep = jnp.exp2((old - new) * (SCALING * LOG2E))
    m_ref[0:1, cols] = new
    total = l_ref[0:1, cols] * keep
    out = acc_ref[:, cols] * keep
    for s, vt_ref in zip(scores, vt_refs, strict=True):
        p = jnp.exp2((s - new) * (SCALING * LOG2E))
        total = total + jnp.sum(p, axis=0, keepdims=True)
        out = out + jnp.dot(vt_ref[...], p.astype(BF16), preferred_element_type=F32)
    l_ref[0:1, cols] = total
    acc_ref[:, cols] = out


def attend_kernel(latents, first, last, tok, beats, *refs):
    n_kv = len(latents)
    q_ref, kv_refs = refs[0], refs[1:1 + n_kv]
    at = 1 + n_kv
    if not first:
        m_in, l_in, acc_in = refs[at:at + 3]
        at += 3
    at += beats
    if last:
        out_ref = refs[at]
        at += 1
    m_ref, l_ref, acc_ref = refs[at:at + 3]
    vt_refs = refs[at + 3:]
    if first:
        m_ref[...] = jnp.full(m_ref.shape, -1e30, F32)
        l_ref[...] = jnp.zeros(l_ref.shape, F32)
        acc_ref[...] = jnp.zeros(acc_ref.shape, F32)
    else:
        m_ref[...] = m_in[...]
        l_ref[...] = l_in[...]
        acc_ref[...] = acc_in[...]
    for kv_ref, vt_ref in zip(kv_refs, vt_refs, strict=True):
        vt_ref[...] = jnp.transpose(kv_ref[:, HEAD:])
    queries = q_ref.shape[0]
    width = 256
    if last:
        for i in range(0, queries, width):
            attend_block(q_ref, kv_refs, vt_refs, m_ref, l_ref, acc_ref, slice(i, i + width), latents)
        for h in range(queries // tok):
            cols = slice(h * tok, (h + 1) * tok)
            done = acc_ref[:, cols] / l_ref[0:1, cols]
            out_ref[:, h * HEAD:(h + 1) * HEAD] = jnp.transpose(done).astype(BF16)
    else:

        @pl.loop(0, queries // width)
        def _(i):
            cols = pl.ds(pl.multiple_of(i * width, width), width)
            attend_block(q_ref, kv_refs, vt_refs, m_ref, l_ref, acc_ref, cols, latents)


def attend(q, chunks, state, tok, beat=None, last=False):
    queries = q.shape[0]
    first = state is None
    latents = [tok] * len(chunks)
    shapes = [
        jax.ShapeDtypeStruct((8, queries), F32),
        jax.ShapeDtypeStruct((8, queries), F32),
        jax.ShapeDtypeStruct((HEAD, queries), F32),
    ]
    rows = sum(c.shape[0] for c in chunks)
    turned = [pltpu.VMEM((HEAD, c.shape[0]), BF16) for c in chunks]
    cost = pl.CostEstimate(
        flops=4 * rows * queries * HEAD, transcendentals=rows * queries, bytes_accessed=1 << 20
    )
    operands = [q, *chunks] + ([] if first else list(state)) + ([] if beat is None else [beat])
    kernel = functools.partial(attend_kernel, latents, first, last, tok, beat is not None)
    if last:
        return pl.pallas_call(
            kernel,
            out_shape=jax.ShapeDtypeStruct((tok, queries // tok * HEAD), BF16),
            in_specs=[VM] * len(operands),
            out_specs=VM,
            scratch_shapes=[*[pltpu.VMEM(s.shape, s.dtype) for s in shapes], *turned],
            cost_estimate=cost,
            compiler_params=pltpu.CompilerParams(vmem_limit_bytes=16 << 20),
            name="attend_last",
        )(*operands)
    return pl.pallas_call(
        kernel,
        out_shape=shapes,
        in_specs=[VM] * len(operands),
        out_specs=[VM] * 3,
        scratch_shapes=turned,
        input_output_aliases={} if first else {1 + len(chunks) + i: i for i in range(3)},
        cost_estimate=cost,
        compiler_params=pltpu.CompilerParams(vmem_limit_bytes=16 << 20),
        name="attend",
    )(*operands)


def shifted(x, axis, by):
    n = lax.axis_size(axis)
    return lax.ppermute(x, axis, [(i, (i + by) % n) for i in range(n)])


def along_ring(x, by):
    n_sp, n_tp = lax.axis_size("sp"), lax.axis_size("tp")
    pairs = []
    for z in range(n_sp):
        for t in range(n_tp):
            to = (z + (by if t % 2 else -by)) % n_sp
            pairs.append((z * n_tp + t, to * n_tp + t))
    return lax.ppermute(x, ("sp", "tp"), pairs)


def other_core(x):
    n = lax.axis_size("tp")
    return lax.ppermute(x, "tp", [(i, i ^ 1) for i in range(n)])


def body(
    latent, context, cond_latent, cond_context, w_shift, w_scale, w_gate, norm_gain,
    w_query, w_key, w_value, q_gain, k_gain, w_out,
):
    seq_index = lax.axis_index("sp")
    n_sp = lax.axis_size("sp")
    tp_index = lax.axis_index("tp")
    mod_rows, mod_cols = w_shift.shape
    tok, width = latent.shape
    ctx = context.shape[0]

    n_tp = lax.axis_size("tp")
    pieces = mod_cols // 128
    lines = -(-5 * pieces // 8) * 8
    partial_mod = pl.pallas_call(
        modulation_kernel,
        out_shape=jax.ShapeDtypeStruct((n_sp, 8 * pieces, 128), BF16),
        in_specs=[pl.BlockSpec(memory_space=pl.ANY)] * 5,
        out_specs=VM,
        scratch_shapes=[
            pltpu.VMEM((2, width // 128, 128), BF16),
            pltpu.VMEM((2, width // 128, 128), F32),
            pltpu.VMEM((3, mod_rows, mod_cols), BF16),
            pltpu.SemaphoreType.DMA((5,)),
        ],
        compiler_params=pltpu.CompilerParams(vmem_limit_bytes=60 << 20),
        name="modulation",
    )(cond_latent.reshape(-1, 128), cond_context.reshape(-1, 128), w_scale, w_shift, w_gate)
    gathered = lax.all_to_all(partial_mod, "sp", split_axis=0, concat_axis=0, tiled=True)
    rx, rc, w_kv = pl.pallas_call(
        prepare_kernel,
        out_shape=[
            jax.ShapeDtypeStruct((tok, 128), F32),
            jax.ShapeDtypeStruct((ctx, 128), F32),
            jax.ShapeDtypeStruct((width, 2 * HEAD), BF16),
        ],
        in_specs=[VM] * 4,
        out_specs=[VM] * 3,
        compiler_params=pltpu.CompilerParams(vmem_limit_bytes=32 << 20),
        cost_estimate=pl.CostEstimate(flops=1 << 30, transcendentals=0, bytes_accessed=12 << 20),
        name="prepare",
    )(latent, context, w_key, w_value)
    positions = seq_index * tok + jnp.arange(tok, dtype=jnp.int32)
    freqs = HEAD // 4
    inverse = ROPE_THETA ** (-jnp.arange(freqs, dtype=F32) / freqs)
    row = (positions // GRID_W).astype(F32)[:, None] * inverse
    col = (positions % GRID_W).astype(F32)[:, None] * inverse
    cos = jnp.concatenate([jnp.cos(row), jnp.cos(row), jnp.cos(col), jnp.cos(col)], axis=1)
    sin = jnp.concatenate([-jnp.sin(row), jnp.sin(row), -jnp.sin(col), jnp.sin(col)], axis=1)

    gathered, rx, rc, w_kv, cos, sin = lax.optimization_barrier((gathered, rx, rc, w_kv, cos, sin))
    summed = pl.pallas_call(
        sum_kernel,
        out_shape=jax.ShapeDtypeStruct((lines, 128), F32),
        in_specs=[VM],
        out_specs=VM,
        compiler_params=pltpu.CompilerParams(vmem_limit_bytes=8 << 20),
        cost_estimate=pl.CostEstimate(flops=8 << 30, transcendentals=0, bytes_accessed=1 << 20),
        name="sum_parts",
    )(gathered)
    pair = jnp.stack([summed, other_core(summed)])
    columns = [pair, shifted(pair, "tp", 2), shifted(pair, "tp", -2)]
    columns.append(shifted(pair, "tp", 4))

    kv, normed, gate = pl.pallas_call(
        kv_kernel,
        out_shape=[
            jax.ShapeDtypeStruct((tok + ctx, 2 * HEAD), BF16),
            jax.ShapeDtypeStruct((tok + ctx, width), BF16),
            jax.ShapeDtypeStruct((1, width), F32),
        ],
        in_specs=[VM] * 13,
        out_specs=[VM] * 3,
        scratch_shapes=[
            pltpu.VMEM((tok + ctx, 2 * HEAD), F32),
            pltpu.VMEM((n_tp, lines, 128), F32),
            pltpu.VMEM((8, width), F32),
        ],
        cost_estimate=pl.CostEstimate(flops=2 * tok * width * 256, transcendentals=0, bytes_accessed=1 << 22),
        compiler_params=pltpu.CompilerParams(vmem_limit_bytes=24 << 20),
        name="project_kv",
    )(
        latent, context, rx, rc, *columns, norm_gain.reshape(1, width), w_kv, k_gain.reshape(1, HEAD), cos, sin
    )

    right, left = along_ring(kv, 1), along_ring(kv, -1)
    q = pl.pallas_call(
        q_kernel,
        out_shape=jax.ShapeDtypeStruct((w_query.shape[1] // HEAD * tok, HEAD), BF16),
        in_specs=[VM] * 5,
        out_specs=VM,
        scratch_shapes=[pltpu.VMEM((tok, w_query.shape[1]), F32)],
        cost_estimate=pl.CostEstimate(flops=2 * tok * width * 256, transcendentals=0, bytes_accessed=1 << 22),
        compiler_params=pltpu.CompilerParams(vmem_limit_bytes=24 << 20),
        name="project_q",
    )(normed, w_query, q_gain.reshape(1, HEAD), cos, sin)
    state = attend(q, [kv], None, tok)
    half = n_sp // 2
    for step in range(1, half):
        beat = other_core(state[0]) if step in (1, 3, 5) else None
        right, m = lax.optimization_barrier((right, state[0]))
        left, m = lax.optimization_barrier((left, m))
        state = [m, *state[1:]]
        now = [right, left]
        right = along_ring(right, 1)
        if step + 1 < half:
            left = along_ring(left, -1)
        state = attend(q, now, state, tok, beat=beat)
    attended = attend(q, [right], state, tok, last=True)

    n_x = lax.axis_size("tp") // 2
    core, chip = tp_index % 2, tp_index // 2
    share = tok // (2 * n_x)
    parts = attended.reshape(n_x, 2, share, attended.shape[1])
    parts = jnp.concatenate([parts, parts], axis=0)
    parts = lax.dynamic_slice_in_dim(parts, chip, n_x, 0)
    mine = lax.dynamic_index_in_dim(parts, core, 1, keepdims=False)
    theirs = lax.dynamic_index_in_dim(parts, 1 - core, 1, keepdims=False)
    far, near = (2,), (1, 3, 0)

    def product(side, which):
        rows = jnp.concatenate([side[i] for i in which]) if len(which) > 1 else side[which[0]]
        return jnp.dot(rows, w_out, preferred_element_type=F32)

    far_sent = other_core(product(theirs, far).astype(BF16))
    own_far, own_near, their_near = lax.optimization_barrier(
        (product(mine, far), product(mine, near), product(theirs, near).astype(BF16))
    )
    far_sum = (own_far + far_sent.astype(F32)).astype(BF16)
    their_near, far_sum = lax.optimization_barrier((their_near, far_sum))
    near_sent = other_core(their_near)
    h = width // 2
    from_left = shifted(far_sum[:, :h], "tp", 2)
    from_right = shifted(far_sum[:, h:], "tp", -2)
    near_sum = own_near + near_sent.astype(F32)
    nxt, prv, own = (near_sum[i * share:(i + 1) * share] for i in range(3))
    halves = (nxt[:, h:].astype(BF16), prv[:, :h].astype(BF16))
    a1 = shifted(halves[0], "tp", 2)
    b0 = shifted(halves[1], "tp", -2)
    joined = ((nxt[:, :h] + from_left.astype(F32)).astype(BF16), (prv[:, h:] + from_right.astype(F32)).astype(BF16))
    a0 = shifted(joined[0], "tp", 2)
    b1 = shifted(joined[1], "tp", -2)
    own, a0, a1, b0, b1 = lax.optimization_barrier((own, a0, a1, b0, b1))
    left_half = own[:, :h] + a0.astype(F32) + b0.astype(F32)
    right_half = own[:, h:] + a1.astype(F32) + b1.astype(F32)
    return (gate * jnp.concatenate([left_half, right_half], axis=1)).astype(BF16)


def solution(mesh):
    placed = (
        P(("grp", "sp"), None),
        P(("grp", "sp"), None),
        P("grp"),
        P(),
        P("sp", "tp"),
        P("sp", "tp"),
        P("sp", "tp"),
        P(),
        P(None, "tp"),
        P(None, "tp"),
        P(None, "tp"),
        P(),
        P(),
        P("tp", None),
    )
    return jax.shard_map(
        body, mesh=mesh, in_specs=placed, out_specs=P(("grp", "sp", "tp"), None), check_vma=False
    )
```

```python
import functools

import jax
import jax.numpy as jnp
from jax import lax
from jax.experimental import pallas as pl
from jax.experimental.pallas import tpu as pltpu
from jax.sharding import PartitionSpec as P


HEAD = 128
GRID_W = 64
EPS = 1e-06
CONTEXT_LIFT = 1.5
ROPE_THETA = 10000.0
SCALING = HEAD ** -0.5
LOG2E = 1.4426950408889634


BF16 = jnp.bfloat16
F32 = jnp.float32
VM = pl.BlockSpec(memory_space=pltpu.VMEM)


def rotate_rows(v, cos, sin):
    lane = lax.broadcasted_iota(jnp.int32, v.shape, 1)
    quarter = HEAD // 4
    partner = jnp.where(
        lane % (2 * quarter) < quarter,
        pltpu.roll(v, HEAD - quarter, 1),
        pltpu.roll(v, quarter, 1),
    )
    return v * cos + partner * sin


def rms_head(v, gain):
    return v * lax.rsqrt(jnp.mean(v * v, axis=-1, keepdims=True) + EPS) * gain


def modulation_kernel(lat_hbm, ctx_hbm, scale_hbm, shift_hbm, gate_hbm, out_ref, cond_ref, act_ref, w_ref, sems):
    conds = [
        pltpu.make_async_copy(c, cond_ref.at[i], sems.at[3 + i]) for i, c in enumerate((lat_hbm, ctx_hbm))
    ]
    copies = [
        pltpu.make_async_copy(w, w_ref.at[i], sems.at[i])
        for i, w in enumerate((scale_hbm, shift_hbm, gate_hbm))
    ]
    for c in conds + copies:
        c.start()
    lines = w_ref.shape[1] // 128
    first = lax.axis_index("sp") * lines
    act = []
    for i, c in enumerate(conds):
        c.wait()
        v = cond_ref[i].astype(F32)
        act_ref[i] = v * jax.nn.sigmoid(v)
        act.append(jnp.concatenate([act_ref[i, pl.ds(first + j, 1), :] for j in range(lines)], axis=1))
    act = jnp.concatenate(act, axis=0).astype(BF16)
    pieces = w_ref.shape[2] // 128
    rows, context_rows = [], []
    for i, c in enumerate(copies):
        c.wait()
        part = jnp.dot(act, w_ref[i], preferred_element_type=F32)
        near = part[0:1].astype(BF16).astype(F32)
        rows += [near, part[0:1] - near]
        if i < 2:
            context_rows.append(part[1:2])
    tile = jnp.concatenate(
        [r[:, 128 * j:128 * j + 128] for r in rows + context_rows for j in range(pieces)], axis=0
    ).astype(BF16)
    for i in range(out_ref.shape[0]):
        out_ref[i] = tile


def sum_kernel(in_ref, out_ref):
    total = in_ref[0].astype(F32)
    for i in range(1, in_ref.shape[0]):
        total = total + in_ref[i].astype(F32)
    pieces = in_ref.shape[1] // 8
    for i in range(3):
        at = 2 * i * pieces
        out_ref[i * pieces:(i + 1) * pieces, :] = total[at:at + pieces] + total[at + pieces:at + 2 * pieces]
    out_ref[3 * pieces:5 * pieces, :] = total[6 * pieces:8 * pieces]
    out_ref[5 * pieces:, :] = jnp.zeros((out_ref.shape[0] - 5 * pieces, 128), F32)


def prepare_kernel(x_ref, c_ref, wk_ref, wv_ref, rx_ref, rc_ref, w_ref):
    tok, width = x_ref.shape
    step = 16

    def rows_of(src, dst, rows):
        total = jnp.zeros((step, 128), F32)
        for j in range(width // 128):
            v = src[rows, 128 * j:128 * j + 128].astype(F32)
            total = total + v * v
        r = lax.rsqrt(jnp.sum(total, axis=-1, keepdims=True) / width + EPS)
        dst[rows, :] = jnp.broadcast_to(r, (step, 128))

    @pl.loop(0, tok // step)
    def _(i):
        rows_of(x_ref, rx_ref, pl.ds(pl.multiple_of(i * step, step), step))

    for i in range(c_ref.shape[0] // step):
        rows_of(c_ref, rc_ref, pl.ds(i * step, step))

    @pl.loop(0, w_ref.shape[0] // 256)
    def _(i):
        rows = pl.ds(pl.multiple_of(i * 256, 256), 256)
        w_ref[rows, :HEAD] = wk_ref[rows, :]
        w_ref[rows, HEAD:] = wv_ref[rows, :]


def kv_kernel(
    x_ref, c_ref, rx_ref, rc_ref, own_ref, m1_ref, m3_ref, m2_ref, gain_ref, w_ref, g_ref, cos_ref, sin_ref,
    kv_ref, nm_ref, gate_ref, both_ref, mod_ref, ab_ref,
):
    tok, width = x_ref.shape
    ctx = c_ref.shape[0]
    n_tp = lax.axis_size("tp")
    chip, core = lax.axis_index("tp") // 2, lax.axis_index("tp") % 2
    n_x = n_tp // 2
    for back, ref in ((0, own_ref), (1, m1_ref), (3, m3_ref), (2, m2_ref)):
        source = lax.rem(chip + n_x - back, n_x)
        for c in range(2):
            mod_ref[2 * source + lax.rem(core + c, 2)] = ref[c]
    pieces = width // n_tp // 128
    for t in range(n_tp):
        for p in range(pieces):
            cs = slice((t * pieces + p) * 128, (t * pieces + p + 1) * 128)
            piece = [mod_ref[t, i * pieces + p:i * pieces + p + 1, :] for i in range(5)]
            gain = gain_ref[:, cs]
            ab_ref[0:1, cs] = gain * (1.0 + piece[0])
            ab_ref[1:2, cs] = piece[1]
            gate_ref[:, cs] = piece[2]
            ab_ref[2:3, cs] = gain * (1.0 + piece[3])
            ab_ref[3:4, cs] = piece[4]

    chunk, step = width // 4, 64
    both = None
    for k in range(0, width, chunk):
        for j in range(k, k + chunk, 128):
            cs = slice(j, j + 128)
            for i in range(0, tok, step):
                rows = slice(i, i + step)
                v = x_ref[rows, cs].astype(F32) * rx_ref[rows, :]
                nm_ref[rows, cs] = (v * ab_ref[0:1, cs] + ab_ref[1:2, cs]).astype(BF16)
            v = c_ref[:, cs].astype(F32) * rc_ref[...]
            nm_ref[tok:tok + ctx, cs] = (v * ab_ref[2:3, cs] + ab_ref[3:4, cs]).astype(BF16)
        part = jnp.dot(nm_ref[:, k:k + chunk], w_ref[k:k + chunk, :], preferred_element_type=F32)
        both = part if both is None else both + part
    both_ref[...] = both
    kv_ref[:, HEAD:] = both_ref[:, HEAD:].astype(BF16)
    gain = g_ref[...]
    tile = 128

    @pl.loop(0, tok // tile)
    def _(i):
        rows = pl.ds(pl.multiple_of(i * tile, tile), tile)
        k = rotate_rows(rms_head(both_ref[rows, :HEAD], gain), cos_ref[rows, :], sin_ref[rows, :])
        kv_ref[rows, :HEAD] = k.astype(BF16)

    kv_ref[tok:tok + ctx, :HEAD] = rms_head(both_ref[tok:tok + ctx, :HEAD], gain).astype(BF16)


def q_kernel(nm_ref, w_ref, g_ref, cos_ref, sin_ref, q_ref, both_ref):
    tok = cos_ref.shape[0]
    heads = w_ref.shape[1] // HEAD
    gain = g_ref[...]
    tile = 128
    both_ref[...] = jnp.dot(nm_ref[:tok, :], w_ref[...], preferred_element_type=F32)

    @pl.loop(0, tok // tile)
    def _(i):
        rows = pl.ds(pl.multiple_of(i * tile, tile), tile)
        for h in range(heads):
            v = rotate_rows(
                rms_head(both_ref[rows, h * HEAD:(h + 1) * HEAD], gain), cos_ref[rows, :], sin_ref[rows, :]
            )
            q_ref[pl.ds(pl.multiple_of(h * tok + i * tile, tile), tile), :] = v.astype(BF16)


def attend_block(q_ref, kv_refs, vt_refs, m_ref, l_ref, acc_ref, cols, latents):
    q = q_ref[cols, :]
    scores = []
    for kv_ref, lat in zip(kv_refs, latents, strict=True):
        s = lax.dot_general(kv_ref[:, :HEAD], q, (((1,), (1,)), ((), ())), preferred_element_type=F32)
        if lat < kv_ref.shape[0]:
            s = jnp.concatenate([s[:lat], s[lat:] + CONTEXT_LIFT / SCALING], axis=0)
        scores.append(s)
    old = m_ref[0:1, cols]
    new = old
    for s in scores:
        new = jnp.maximum(new, jnp.max(s, axis=0, keepdims=True))
    keep = jnp.exp2((old - new) * (SCALING * LOG2E))
    m_ref[0:1, cols] = new
    total = l_ref[0:1, cols] * keep
    out = acc_ref[:, cols] * keep
    for s, vt_ref in zip(scores, vt_refs, strict=True):
        p = jnp.exp2((s - new) * (SCALING * LOG2E))
        total = total + jnp.sum(p, axis=0, keepdims=True)
        out = out + jnp.dot(vt_ref[...], p.astype(BF16), preferred_element_type=F32)
    l_ref[0:1, cols] = total
    acc_ref[:, cols] = out


def attend_kernel(latents, first, last, tok, *refs):
    n_kv = len(latents)
    q_ref, kv_refs = refs[0], refs[1:1 + n_kv]
    at = 1 + n_kv
    if not first:
        m_in, l_in, acc_in = refs[at:at + 3]
        at += 3
    if last:
        out_ref = refs[at]
        at += 1
    m_ref, l_ref, acc_ref = refs[at:at + 3]
    vt_refs = refs[at + 3:]
    if first:
        m_ref[...] = jnp.full(m_ref.shape, -1e30, F32)
        l_ref[...] = jnp.zeros(l_ref.shape, F32)
        acc_ref[...] = jnp.zeros(acc_ref.shape, F32)
    else:
        m_ref[...] = m_in[...]
        l_ref[...] = l_in[...]
        acc_ref[...] = acc_in[...]
    for kv_ref, vt_ref in zip(kv_refs, vt_refs, strict=True):
        vt_ref[...] = jnp.transpose(kv_ref[:, HEAD:])
    queries = q_ref.shape[0]
    width = 256
    if last:
        for i in range(0, queries, width):
            attend_block(q_ref, kv_refs, vt_refs, m_ref, l_ref, acc_ref, slice(i, i + width), latents)
        for h in range(queries // tok):
            cols = slice(h * tok, (h + 1) * tok)
            done = acc_ref[:, cols] / l_ref[0:1, cols]
            out_ref[:, h * HEAD:(h + 1) * HEAD] = jnp.transpose(done).astype(BF16)
    else:

        @pl.loop(0, queries // width)
        def _(i):
            cols = pl.ds(pl.multiple_of(i * width, width), width)
            attend_block(q_ref, kv_refs, vt_refs, m_ref, l_ref, acc_ref, cols, latents)


def attend(q, chunks, state, tok, last=False):
    queries = q.shape[0]
    first = state is None
    latents = [tok] * len(chunks)
    shapes = [
        jax.ShapeDtypeStruct((8, queries), F32),
        jax.ShapeDtypeStruct((8, queries), F32),
        jax.ShapeDtypeStruct((HEAD, queries), F32),
    ]
    rows = sum(c.shape[0] for c in chunks)
    turned = [pltpu.VMEM((HEAD, c.shape[0]), BF16) for c in chunks]
    cost = pl.CostEstimate(
        flops=4 * rows * queries * HEAD, transcendentals=rows * queries, bytes_accessed=1 << 20
    )
    operands = [q, *chunks] + ([] if first else list(state))
    kernel = functools.partial(attend_kernel, latents, first, last, tok)
    if last:
        return pl.pallas_call(
            kernel,
            out_shape=jax.ShapeDtypeStruct((tok, queries // tok * HEAD), BF16),
            in_specs=[VM] * len(operands),
            out_specs=VM,
            scratch_shapes=[*[pltpu.VMEM(s.shape, s.dtype) for s in shapes], *turned],
            cost_estimate=cost,
            compiler_params=pltpu.CompilerParams(vmem_limit_bytes=16 << 20),
            name="attend_last",
        )(*operands)
    return pl.pallas_call(
        kernel,
        out_shape=shapes,
        in_specs=[VM] * len(operands),
        out_specs=[VM] * 3,
        scratch_shapes=turned,
        input_output_aliases={} if first else {1 + len(chunks) + i: i for i in range(3)},
        cost_estimate=cost,
        compiler_params=pltpu.CompilerParams(vmem_limit_bytes=16 << 20),
        name="attend",
    )(*operands)


def shifted(x, axis, by):
    n = lax.axis_size(axis)
    return lax.ppermute(x, axis, [(i, (i + by) % n) for i in range(n)])


def along_ring(x, by):
    n_sp, n_tp = lax.axis_size("sp"), lax.axis_size("tp")
    pairs = []
    for z in range(n_sp):
        for t in range(n_tp):
            to = (z + (by if t % 2 else -by)) % n_sp
            pairs.append((z * n_tp + t, to * n_tp + t))
    return lax.ppermute(x, ("sp", "tp"), pairs)


def other_core(x):
    n = lax.axis_size("tp")
    return lax.ppermute(x, "tp", [(i, i ^ 1) for i in range(n)])


def body(
    latent, context, cond_latent, cond_context, w_shift, w_scale, w_gate, norm_gain,
    w_query, w_key, w_value, q_gain, k_gain, w_out,
):
    seq_index = lax.axis_index("sp")
    n_sp = lax.axis_size("sp")
    tp_index = lax.axis_index("tp")
    mod_rows, mod_cols = w_shift.shape
    tok, width = latent.shape
    ctx = context.shape[0]

    n_tp = lax.axis_size("tp")
    pieces = mod_cols // 128
    lines = -(-5 * pieces // 8) * 8
    partial_mod = pl.pallas_call(
        modulation_kernel,
        out_shape=jax.ShapeDtypeStruct((n_sp, 8 * pieces, 128), BF16),
        in_specs=[pl.BlockSpec(memory_space=pl.ANY)] * 5,
        out_specs=VM,
        scratch_shapes=[
            pltpu.VMEM((2, width // 128, 128), BF16),
            pltpu.VMEM((2, width // 128, 128), F32),
            pltpu.VMEM((3, mod_rows, mod_cols), BF16),
            pltpu.SemaphoreType.DMA((5,)),
        ],
        compiler_params=pltpu.CompilerParams(vmem_limit_bytes=60 << 20),
        name="modulation",
    )(cond_latent.reshape(-1, 128), cond_context.reshape(-1, 128), w_scale, w_shift, w_gate)
    gathered = lax.all_to_all(partial_mod, "sp", split_axis=0, concat_axis=0, tiled=True)
    rx, rc, w_kv = pl.pallas_call(
        prepare_kernel,
        out_shape=[
            jax.ShapeDtypeStruct((tok, 128), F32),
            jax.ShapeDtypeStruct((ctx, 128), F32),
            jax.ShapeDtypeStruct((width, 2 * HEAD), BF16),
        ],
        in_specs=[VM] * 4,
        out_specs=[VM] * 3,
        compiler_params=pltpu.CompilerParams(vmem_limit_bytes=32 << 20),
        cost_estimate=pl.CostEstimate(flops=1 << 30, transcendentals=0, bytes_accessed=12 << 20),
        name="prepare",
    )(latent, context, w_key, w_value)
    positions = seq_index * tok + jnp.arange(tok, dtype=jnp.int32)
    freqs = HEAD // 4
    inverse = ROPE_THETA ** (-jnp.arange(freqs, dtype=F32) / freqs)
    row = (positions // GRID_W).astype(F32)[:, None] * inverse
    col = (positions % GRID_W).astype(F32)[:, None] * inverse
    cos = jnp.concatenate([jnp.cos(row), jnp.cos(row), jnp.cos(col), jnp.cos(col)], axis=1)
    sin = jnp.concatenate([-jnp.sin(row), jnp.sin(row), -jnp.sin(col), jnp.sin(col)], axis=1)

    gathered, rx, rc, w_kv, cos, sin = lax.optimization_barrier((gathered, rx, rc, w_kv, cos, sin))
    summed = pl.pallas_call(
        sum_kernel,
        out_shape=jax.ShapeDtypeStruct((lines, 128), F32),
        in_specs=[VM],
        out_specs=VM,
        compiler_params=pltpu.CompilerParams(vmem_limit_bytes=8 << 20),
        cost_estimate=pl.CostEstimate(flops=8 << 30, transcendentals=0, bytes_accessed=1 << 20),
        name="sum_parts",
    )(gathered)
    pair = jnp.stack([summed, other_core(summed)])
    columns = [pair, shifted(pair, "tp", 2), shifted(pair, "tp", -2)]
    columns.append(shifted(pair, "tp", 4))

    kv, normed, gate = pl.pallas_call(
        kv_kernel,
        out_shape=[
            jax.ShapeDtypeStruct((tok + ctx, 2 * HEAD), BF16),
            jax.ShapeDtypeStruct((tok + ctx, width), BF16),
            jax.ShapeDtypeStruct((1, width), F32),
        ],
        in_specs=[VM] * 13,
        out_specs=[VM] * 3,
        scratch_shapes=[
            pltpu.VMEM((tok + ctx, 2 * HEAD), F32),
            pltpu.VMEM((n_tp, lines, 128), F32),
            pltpu.VMEM((8, width), F32),
        ],
        cost_estimate=pl.CostEstimate(flops=2 * tok * width * 256, transcendentals=0, bytes_accessed=1 << 22),
        compiler_params=pltpu.CompilerParams(vmem_limit_bytes=24 << 20),
        name="project_kv",
    )(
        latent, context, rx, rc, *columns, norm_gain.reshape(1, width), w_kv, k_gain.reshape(1, HEAD), cos, sin
    )

    right, left = along_ring(kv, 1), along_ring(kv, -1)
    q = pl.pallas_call(
        q_kernel,
        out_shape=jax.ShapeDtypeStruct((w_query.shape[1] // HEAD * tok, HEAD), BF16),
        in_specs=[VM] * 5,
        out_specs=VM,
        scratch_shapes=[pltpu.VMEM((tok, w_query.shape[1]), F32)],
        cost_estimate=pl.CostEstimate(flops=2 * tok * width * 256, transcendentals=0, bytes_accessed=1 << 22),
        compiler_params=pltpu.CompilerParams(vmem_limit_bytes=24 << 20),
        name="project_q",
    )(normed, w_query, q_gain.reshape(1, HEAD), cos, sin)
    state = attend(q, [kv], None, tok)
    half = n_sp // 2
    for step in range(1, half):
        right, m = lax.optimization_barrier((right, state[0]))
        now, right = right, along_ring(right, 1)
        state = attend(q, [now], [m, *state[1:]], tok)
        left, m = lax.optimization_barrier((left, state[0]))
        now = left
        if step + 1 < half:
            left = along_ring(left, -1)
        state = attend(q, [now], [m, *state[1:]], tok)
    attended = attend(q, [right], state, tok, last=True)

    n_x = lax.axis_size("tp") // 2
    core, chip = tp_index % 2, tp_index // 2
    share = tok // (2 * n_x)
    parts = attended.reshape(n_x, 2, share, attended.shape[1])
    parts = jnp.concatenate([parts, parts], axis=0)
    parts = lax.dynamic_slice_in_dim(parts, chip, n_x, 0)
    mine = lax.dynamic_index_in_dim(parts, core, 1, keepdims=False)
    theirs = lax.dynamic_index_in_dim(parts, 1 - core, 1, keepdims=False)
    far, near = (2,), (1, 3, 0)

    def product(side, which):
        rows = jnp.concatenate([side[i] for i in which]) if len(which) > 1 else side[which[0]]
        return jnp.dot(rows, w_out, preferred_element_type=F32)

    far_sent = other_core(product(theirs, far).astype(BF16))
    far_sum = (product(mine, far) + far_sent.astype(F32)).astype(BF16)
    theirs, far_sum = lax.optimization_barrier((theirs, far_sum))
    near_sent = other_core(product(theirs, near).astype(BF16))
    h = width // 2
    from_left = shifted(far_sum[:, :h], "tp", 2)
    from_right = shifted(far_sum[:, h:], "tp", -2)
    near_sum = product(mine, near) + near_sent.astype(F32)
    nxt, prv, own = (near_sum[i * share:(i + 1) * share] for i in range(3))
    halves = (nxt[:, h:].astype(BF16), prv[:, :h].astype(BF16))
    a1 = shifted(halves[0], "tp", 2)
    b0 = shifted(halves[1], "tp", -2)
    joined = ((nxt[:, :h] + from_left.astype(F32)).astype(BF16), (prv[:, h:] + from_right.astype(F32)).astype(BF16))
    a0 = shifted(joined[0], "tp", 2)
    b1 = shifted(joined[1], "tp", -2)
    own, a0, a1, b0, b1 = lax.optimization_barrier((own, a0, a1, b0, b1))
    left_half = own[:, :h] + a0.astype(F32) + b0.astype(F32)
    right_half = own[:, h:] + a1.astype(F32) + b1.astype(F32)
    return (gate * jnp.concatenate([left_half, right_half], axis=1)).astype(BF16)


def solution(mesh):
    placed = (
        P(("grp", "sp"), None),
        P(("grp", "sp"), None),
        P("grp"),
        P(),
        P("sp", "tp"),
        P("sp", "tp"),
        P("sp", "tp"),
        P(),
        P(None, "tp"),
        P(None, "tp"),
        P(None, "tp"),
        P(),
        P(),
        P("tp", None),
    )
    return jax.shard_map(
        body, mesh=mesh, in_specs=placed, out_specs=P(("grp", "sp", "tp"), None), check_vma=False
    )
```

```python
import functools

import jax
import jax.numpy as jnp
from jax import lax
from jax.experimental import pallas as pl
from jax.experimental.pallas import tpu as pltpu
from jax.sharding import PartitionSpec as P


HEAD = 128
GRID_W = 64
EPS = 1e-06
CONTEXT_LIFT = 1.5
ROPE_THETA = 10000.0
SCALING = HEAD ** -0.5
LOG2E = 1.4426950408889634


BF16 = jnp.bfloat16
F32 = jnp.float32
VM = pl.BlockSpec(memory_space=pltpu.VMEM)


def rotate_rows(v, cos, sin):
    lane = lax.broadcasted_iota(jnp.int32, v.shape, 1)
    quarter = HEAD // 4
    partner = jnp.where(
        lane % (2 * quarter) < quarter,
        pltpu.roll(v, HEAD - quarter, 1),
        pltpu.roll(v, quarter, 1),
    )
    return v * cos + partner * sin


def rms_head(v, gain):
    return v * lax.rsqrt(jnp.mean(v * v, axis=-1, keepdims=True) + EPS) * gain


def modulation_kernel(lat_hbm, ctx_hbm, scale_hbm, shift_hbm, gate_hbm, out_ref, cond_ref, act_ref, w_ref, sems):
    conds = [
        pltpu.make_async_copy(c, cond_ref.at[i], sems.at[3 + i]) for i, c in enumerate((lat_hbm, ctx_hbm))
    ]
    copies = [
        pltpu.make_async_copy(w, w_ref.at[i], sems.at[i])
        for i, w in enumerate((scale_hbm, shift_hbm, gate_hbm))
    ]
    for c in conds + copies:
        c.start()
    lines = w_ref.shape[1] // 128
    first = lax.axis_index("sp") * lines
    act = []
    for i, c in enumerate(conds):
        c.wait()
        v = cond_ref[i].astype(F32)
        act_ref[i] = v * jax.nn.sigmoid(v)
        act.append(jnp.concatenate([act_ref[i, pl.ds(first + j, 1), :] for j in range(lines)], axis=1))
    act = jnp.concatenate(act, axis=0).astype(BF16)
    pieces = w_ref.shape[2] // 128
    rows, context_rows = [], []
    for i, c in enumerate(copies):
        c.wait()
        part = jnp.dot(act, w_ref[i], preferred_element_type=F32)
        near = part[0:1].astype(BF16).astype(F32)
        rows += [near, part[0:1] - near]
        if i < 2:
            context_rows.append(part[1:2])
    tile = jnp.concatenate(
        [r[:, 128 * j:128 * j + 128] for r in rows + context_rows for j in range(pieces)], axis=0
    ).astype(BF16)
    for i in range(out_ref.shape[0]):
        out_ref[i] = tile


def sum_kernel(in_ref, out_ref):
    total = in_ref[0].astype(F32)
    for i in range(1, in_ref.shape[0]):
        total = total + in_ref[i].astype(F32)
    pieces = in_ref.shape[1] // 8
    for i in range(3):
        at = 2 * i * pieces
        out_ref[i * pieces:(i + 1) * pieces, :] = total[at:at + pieces] + total[at + pieces:at + 2 * pieces]
    out_ref[3 * pieces:5 * pieces, :] = total[6 * pieces:8 * pieces]
    out_ref[5 * pieces:, :] = jnp.zeros((out_ref.shape[0] - 5 * pieces, 128), F32)


def prepare_kernel(x_ref, c_ref, wk_ref, wv_ref, rx_ref, rc_ref, w_ref):
    tok, width = x_ref.shape
    step = 16

    def rows_of(src, dst, rows):
        total = jnp.zeros((step, 128), F32)
        for j in range(width // 128):
            v = src[rows, 128 * j:128 * j + 128].astype(F32)
            total = total + v * v
        r = lax.rsqrt(jnp.sum(total, axis=-1, keepdims=True) / width + EPS)
        dst[rows, :] = jnp.broadcast_to(r, (step, 128))

    @pl.loop(0, tok // step)
    def _(i):
        rows_of(x_ref, rx_ref, pl.ds(pl.multiple_of(i * step, step), step))

    for i in range(c_ref.shape[0] // step):
        rows_of(c_ref, rc_ref, pl.ds(i * step, step))

    @pl.loop(0, w_ref.shape[0] // 256)
    def _(i):
        rows = pl.ds(pl.multiple_of(i * 256, 256), 256)
        w_ref[rows, :HEAD] = wk_ref[rows, :]
        w_ref[rows, HEAD:] = wv_ref[rows, :]


def kv_kernel(
    x_ref, c_ref, rx_ref, rc_ref, own_ref, m1_ref, m3_ref, m2_ref, gain_ref, w_ref, g_ref, cos_ref, sin_ref,
    kv_ref, nm_ref, gate_ref, both_ref, mod_ref, ab_ref,
):
    tok, width = x_ref.shape
    ctx = c_ref.shape[0]
    n_tp = lax.axis_size("tp")
    chip, core = lax.axis_index("tp") // 2, lax.axis_index("tp") % 2
    n_x = n_tp // 2
    for back, ref in ((0, own_ref), (1, m1_ref), (3, m3_ref), (2, m2_ref)):
        source = lax.rem(chip + n_x - back, n_x)
        for c in range(2):
            mod_ref[2 * source + lax.rem(core + c, 2)] = ref[c]
    pieces = width // n_tp // 128
    for t in range(n_tp):
        for p in range(pieces):
            cs = slice((t * pieces + p) * 128, (t * pieces + p + 1) * 128)
            piece = [mod_ref[t, i * pieces + p:i * pieces + p + 1, :] for i in range(5)]
            gain = gain_ref[:, cs]
            ab_ref[0:1, cs] = gain * (1.0 + piece[0])
            ab_ref[1:2, cs] = piece[1]
            gate_ref[:, cs] = piece[2]
            ab_ref[2:3, cs] = gain * (1.0 + piece[3])
            ab_ref[3:4, cs] = piece[4]

    chunk, step = width // 4, 64
    both = None
    for k in range(0, width, chunk):
        for j in range(k, k + chunk, 128):
            cs = slice(j, j + 128)
            for i in range(0, tok, step):
                rows = slice(i, i + step)
                v = x_ref[rows, cs].astype(F32) * rx_ref[rows, :]
                nm_ref[rows, cs] = (v * ab_ref[0:1, cs] + ab_ref[1:2, cs]).astype(BF16)
            v = c_ref[:, cs].astype(F32) * rc_ref[...]
            nm_ref[tok:tok + ctx, cs] = (v * ab_ref[2:3, cs] + ab_ref[3:4, cs]).astype(BF16)
        part = jnp.dot(nm_ref[:, k:k + chunk], w_ref[k:k + chunk, :], preferred_element_type=F32)
        both = part if both is None else both + part
    both_ref[...] = both
    kv_ref[:, HEAD:] = both_ref[:, HEAD:].astype(BF16)
    gain = g_ref[...]
    tile = 128

    @pl.loop(0, tok // tile)
    def _(i):
        rows = pl.ds(pl.multiple_of(i * tile, tile), tile)
        k = rotate_rows(rms_head(both_ref[rows, :HEAD], gain), cos_ref[rows, :], sin_ref[rows, :])
        kv_ref[rows, :HEAD] = k.astype(BF16)

    kv_ref[tok:tok + ctx, :HEAD] = rms_head(both_ref[tok:tok + ctx, :HEAD], gain).astype(BF16)


def q_kernel(nm_ref, w_ref, g_ref, cos_ref, sin_ref, q_ref, both_ref):
    tok = cos_ref.shape[0]
    heads = w_ref.shape[1] // HEAD
    gain = g_ref[...]
    tile = 128
    both_ref[...] = jnp.dot(nm_ref[:tok, :], w_ref[...], preferred_element_type=F32)

    @pl.loop(0, tok // tile)
    def _(i):
        rows = pl.ds(pl.multiple_of(i * tile, tile), tile)
        for h in range(heads):
            v = rotate_rows(
                rms_head(both_ref[rows, h * HEAD:(h + 1) * HEAD], gain), cos_ref[rows, :], sin_ref[rows, :]
            )
            q_ref[pl.ds(pl.multiple_of(h * tok + i * tile, tile), tile), :] = v.astype(BF16)


def attend_block(q_ref, kv_refs, vt_refs, m_ref, l_ref, acc_ref, cols, latents):
    q = q_ref[cols, :]
    scores = []
    for kv_ref, lat in zip(kv_refs, latents, strict=True):
        s = lax.dot_general(kv_ref[:, :HEAD], q, (((1,), (1,)), ((), ())), preferred_element_type=F32)
        if lat < kv_ref.shape[0]:
            s = jnp.concatenate([s[:lat], s[lat:] + CONTEXT_LIFT / SCALING], axis=0)
        scores.append(s)
    old = m_ref[0:1, cols]
    new = old
    for s in scores:
        new = jnp.maximum(new, jnp.max(s, axis=0, keepdims=True))
    keep = jnp.exp2((old - new) * (SCALING * LOG2E))
    m_ref[0:1, cols] = new
    total = l_ref[0:1, cols] * keep
    out = acc_ref[:, cols] * keep
    for s, vt_ref in zip(scores, vt_refs, strict=True):
        p = jnp.exp2((s - new) * (SCALING * LOG2E))
        total = total + jnp.sum(p, axis=0, keepdims=True)
        out = out + jnp.dot(vt_ref[...], p.astype(BF16), preferred_element_type=F32)
    l_ref[0:1, cols] = total
    acc_ref[:, cols] = out


def attend_kernel(latents, first, last, tok, *refs):
    n_kv = len(latents)
    q_ref, kv_refs = refs[0], refs[1:1 + n_kv]
    at = 1 + n_kv
    if not first:
        m_in, l_in, acc_in = refs[at:at + 3]
        at += 3
    if last:
        out_ref = refs[at]
        at += 1
    m_ref, l_ref, acc_ref = refs[at:at + 3]
    vt_refs = refs[at + 3:]
    if first:
        m_ref[...] = jnp.full(m_ref.shape, -1e30, F32)
        l_ref[...] = jnp.zeros(l_ref.shape, F32)
        acc_ref[...] = jnp.zeros(acc_ref.shape, F32)
    else:
        m_ref[...] = m_in[...]
        l_ref[...] = l_in[...]
        acc_ref[...] = acc_in[...]
    for kv_ref, vt_ref in zip(kv_refs, vt_refs, strict=True):
        vt_ref[...] = jnp.transpose(kv_ref[:, HEAD:])
    queries = q_ref.shape[0]
    if last:
        attend_block(q_ref, kv_refs, vt_refs, m_ref, l_ref, acc_ref, slice(0, queries), latents)
        for h in range(queries // tok):
            cols = slice(h * tok, (h + 1) * tok)
            done = acc_ref[:, cols] / l_ref[0:1, cols]
            out_ref[:, h * HEAD:(h + 1) * HEAD] = jnp.transpose(done).astype(BF16)
    else:


        @pl.loop(0, queries // tok)
        def _(i):
            cols = pl.ds(pl.multiple_of(i * tok, tok), tok)
            attend_block(q_ref, kv_refs, vt_refs, m_ref, l_ref, acc_ref, cols, latents)


def attend(q, chunks, state, tok, last=False):
    queries = q.shape[0]
    first = state is None
    latents = [tok] * len(chunks)
    shapes = [
        jax.ShapeDtypeStruct((8, queries), F32),
        jax.ShapeDtypeStruct((8, queries), F32),
        jax.ShapeDtypeStruct((HEAD, queries), F32),
    ]
    rows = sum(c.shape[0] for c in chunks)
    turned = [pltpu.VMEM((HEAD, c.shape[0]), BF16) for c in chunks]
    cost = pl.CostEstimate(
        flops=4 * rows * queries * HEAD, transcendentals=rows * queries, bytes_accessed=1 << 20
    )
    operands = [q, *chunks] + ([] if first else list(state))
    kernel = functools.partial(attend_kernel, latents, first, last, tok)
    if last:
        return pl.pallas_call(
            kernel,
            out_shape=jax.ShapeDtypeStruct((tok, queries // tok * HEAD), BF16),
            in_specs=[VM] * len(operands),
            out_specs=VM,
            scratch_shapes=[*[pltpu.VMEM(s.shape, s.dtype) for s in shapes], *turned],
            cost_estimate=cost,
            compiler_params=pltpu.CompilerParams(vmem_limit_bytes=16 << 20),
            name="attend_last",
        )(*operands)
    return pl.pallas_call(
        kernel,
        out_shape=shapes,
        in_specs=[VM] * len(operands),
        out_specs=[VM] * 3,
        scratch_shapes=turned,
        input_output_aliases={} if first else {1 + len(chunks) + i: i for i in range(3)},
        cost_estimate=cost,
        compiler_params=pltpu.CompilerParams(vmem_limit_bytes=16 << 20),
        name="attend",
    )(*operands)


def shifted(x, axis, by):
    n = lax.axis_size(axis)
    return lax.ppermute(x, axis, [(i, (i + by) % n) for i in range(n)])


def along_ring(x, by):
    n_sp, n_tp = lax.axis_size("sp"), lax.axis_size("tp")
    pairs = []
    for z in range(n_sp):
        for t in range(n_tp):
            to = (z + (by if t % 2 else -by)) % n_sp
            pairs.append((z * n_tp + t, to * n_tp + t))
    return lax.ppermute(x, ("sp", "tp"), pairs)


def other_core(x):
    n = lax.axis_size("tp")
    return lax.ppermute(x, "tp", [(i, i ^ 1) for i in range(n)])


def body(
    latent, context, cond_latent, cond_context, w_shift, w_scale, w_gate, norm_gain,
    w_query, w_key, w_value, q_gain, k_gain, w_out,
):
    seq_index = lax.axis_index("sp")
    n_sp = lax.axis_size("sp")
    tp_index = lax.axis_index("tp")
    mod_rows, mod_cols = w_shift.shape
    tok, width = latent.shape
    ctx = context.shape[0]

    n_tp = lax.axis_size("tp")
    pieces = mod_cols // 128
    lines = -(-5 * pieces // 8) * 8
    partial_mod = pl.pallas_call(
        modulation_kernel,
        out_shape=jax.ShapeDtypeStruct((n_sp, 8 * pieces, 128), BF16),
        in_specs=[pl.BlockSpec(memory_space=pl.ANY)] * 5,
        out_specs=VM,
        scratch_shapes=[
            pltpu.VMEM((2, width // 128, 128), BF16),
            pltpu.VMEM((2, width // 128, 128), F32),
            pltpu.VMEM((3, mod_rows, mod_cols), BF16),
            pltpu.SemaphoreType.DMA((5,)),
        ],
        compiler_params=pltpu.CompilerParams(vmem_limit_bytes=60 << 20),
        name="modulation",
    )(cond_latent.reshape(-1, 128), cond_context.reshape(-1, 128), w_scale, w_shift, w_gate)
    gathered = lax.all_to_all(partial_mod, "sp", split_axis=0, concat_axis=0, tiled=True)
    rx, rc, w_kv = pl.pallas_call(
        prepare_kernel,
        out_shape=[
            jax.ShapeDtypeStruct((tok, 128), F32),
            jax.ShapeDtypeStruct((ctx, 128), F32),
            jax.ShapeDtypeStruct((width, 2 * HEAD), BF16),
        ],
        in_specs=[VM] * 4,
        out_specs=[VM] * 3,
        compiler_params=pltpu.CompilerParams(vmem_limit_bytes=32 << 20),
        cost_estimate=pl.CostEstimate(flops=1 << 30, transcendentals=0, bytes_accessed=12 << 20),
        name="prepare",
    )(latent, context, w_key, w_value)
    positions = seq_index * tok + jnp.arange(tok, dtype=jnp.int32)
    freqs = HEAD // 4
    inverse = ROPE_THETA ** (-jnp.arange(freqs, dtype=F32) / freqs)
    row = (positions // GRID_W).astype(F32)[:, None] * inverse
    col = (positions % GRID_W).astype(F32)[:, None] * inverse
    cos = jnp.concatenate([jnp.cos(row), jnp.cos(row), jnp.cos(col), jnp.cos(col)], axis=1)
    sin = jnp.concatenate([-jnp.sin(row), jnp.sin(row), -jnp.sin(col), jnp.sin(col)], axis=1)

    gathered, rx, rc, w_kv, cos, sin = lax.optimization_barrier((gathered, rx, rc, w_kv, cos, sin))
    summed = pl.pallas_call(
        sum_kernel,
        out_shape=jax.ShapeDtypeStruct((lines, 128), F32),
        in_specs=[VM],
        out_specs=VM,
        compiler_params=pltpu.CompilerParams(vmem_limit_bytes=8 << 20),
        cost_estimate=pl.CostEstimate(flops=8 << 30, transcendentals=0, bytes_accessed=1 << 20),
        name="sum_parts",
    )(gathered)
    pair = jnp.stack([summed, other_core(summed)])
    columns = [pair, shifted(pair, "tp", 2), shifted(pair, "tp", -2)]
    columns.append(shifted(pair, "tp", 4))

    kv, normed, gate = pl.pallas_call(
        kv_kernel,
        out_shape=[
            jax.ShapeDtypeStruct((tok + ctx, 2 * HEAD), BF16),
            jax.ShapeDtypeStruct((tok + ctx, width), BF16),
            jax.ShapeDtypeStruct((1, width), F32),
        ],
        in_specs=[VM] * 13,
        out_specs=[VM] * 3,
        scratch_shapes=[
            pltpu.VMEM((tok + ctx, 2 * HEAD), F32),
            pltpu.VMEM((n_tp, lines, 128), F32),
            pltpu.VMEM((8, width), F32),
        ],
        cost_estimate=pl.CostEstimate(flops=2 * tok * width * 256, transcendentals=0, bytes_accessed=1 << 22),
        compiler_params=pltpu.CompilerParams(vmem_limit_bytes=24 << 20),
        name="project_kv",
    )(
        latent, context, rx, rc, *columns, norm_gain.reshape(1, width), w_kv, k_gain.reshape(1, HEAD), cos, sin
    )

    right, left = along_ring(kv, 1), along_ring(kv, -1)
    q = pl.pallas_call(
        q_kernel,
        out_shape=jax.ShapeDtypeStruct((w_query.shape[1] // HEAD * tok, HEAD), BF16),
        in_specs=[VM] * 5,
        out_specs=VM,
        scratch_shapes=[pltpu.VMEM((tok, w_query.shape[1]), F32)],
        cost_estimate=pl.CostEstimate(flops=2 * tok * width * 256, transcendentals=0, bytes_accessed=1 << 22),
        compiler_params=pltpu.CompilerParams(vmem_limit_bytes=24 << 20),
        name="project_q",
    )(normed, w_query, q_gain.reshape(1, HEAD), cos, sin)
    state = attend(q, [kv], None, tok)
    half = n_sp // 2
    for step in range(1, half):
        right, m = lax.optimization_barrier((right, state[0]))
        now, right = right, along_ring(right, 1)
        state = attend(q, [now], [m, *state[1:]], tok)
        left, m = lax.optimization_barrier((left, state[0]))
        now = left
        if step + 1 < half:
            left = along_ring(left, -1)
        state = attend(q, [now], [m, *state[1:]], tok)
    attended = attend(q, [right], state, tok, last=True)

    n_x = lax.axis_size("tp") // 2
    core, chip = tp_index % 2, tp_index // 2
    share = tok // (2 * n_x)
    parts = attended.reshape(n_x, 2, share, attended.shape[1])
    parts = jnp.concatenate([parts, parts], axis=0)
    parts = lax.dynamic_slice_in_dim(parts, chip, n_x, 0)
    mine = lax.dynamic_index_in_dim(parts, core, 1, keepdims=False)
    theirs = lax.dynamic_index_in_dim(parts, 1 - core, 1, keepdims=False)
    far, near = (2,), (1, 3, 0)

    def product(side, which):
        rows = jnp.concatenate([side[i] for i in which]) if len(which) > 1 else side[which[0]]
        return jnp.dot(rows, w_out, preferred_element_type=F32)

    far_sent = other_core(product(theirs, far).astype(BF16))
    far_sum = (product(mine, far) + far_sent.astype(F32)).astype(BF16)
    theirs, far_sum = lax.optimization_barrier((theirs, far_sum))
    near_sent = other_core(product(theirs, near).astype(BF16))
    h = width // 2
    from_left = shifted(far_sum[:, :h], "tp", 2)
    from_right = shifted(far_sum[:, h:], "tp", -2)
    near_sum = product(mine, near) + near_sent.astype(F32)
    nxt, prv, own = (near_sum[i * share:(i + 1) * share] for i in range(3))
    halves = (nxt[:, h:].astype(BF16), prv[:, :h].astype(BF16))
    a1 = shifted(halves[0], "tp", 2)
    b0 = shifted(halves[1], "tp", -2)
    joined = ((nxt[:, :h] + from_left.astype(F32)).astype(BF16), (prv[:, h:] + from_right.astype(F32)).astype(BF16))
    a0 = shifted(joined[0], "tp", 2)
    b1 = shifted(joined[1], "tp", -2)
    own, a0, a1, b0, b1 = lax.optimization_barrier((own, a0, a1, b0, b1))
    left_half = own[:, :h] + a0.astype(F32) + b0.astype(F32)
    right_half = own[:, h:] + a1.astype(F32) + b1.astype(F32)
    return (gate * jnp.concatenate([left_half, right_half], axis=1)).astype(BF16)


def solution(mesh):
    placed = (
        P(("grp", "sp"), None),
        P(("grp", "sp"), None),
        P("grp"),
        P(),
        P("sp", "tp"),
        P("sp", "tp"),
        P("sp", "tp"),
        P(),
        P(None, "tp"),
        P(None, "tp"),
        P(None, "tp"),
        P(),
        P(),
        P("tp", None),
    )
    return jax.shard_map(
        body, mesh=mesh, in_specs=placed, out_specs=P(("grp", "sp", "tp"), None), check_vma=False
    )
```

```python
import functools

import jax
import jax.numpy as jnp
from jax import lax
from jax.experimental import pallas as pl
from jax.experimental.pallas import tpu as pltpu
from jax.sharding import PartitionSpec as P


HEAD = 128
GRID_W = 64
EPS = 1e-06
CONTEXT_LIFT = 1.5
ROPE_THETA = 10000.0
SCALING = HEAD ** -0.5
LOG2E = 1.4426950408889634


BF16 = jnp.bfloat16
F32 = jnp.float32
VM = pl.BlockSpec(memory_space=pltpu.VMEM)


def rotate_rows(v, cos, sin):
    lane = lax.broadcasted_iota(jnp.int32, v.shape, 1)
    quarter = HEAD // 4
    partner = jnp.where(
        lane % (2 * quarter) < quarter,
        pltpu.roll(v, HEAD - quarter, 1),
        pltpu.roll(v, quarter, 1),
    )
    return v * cos + partner * sin


def rms_head(v, gain):
    return v * lax.rsqrt(jnp.mean(v * v, axis=-1, keepdims=True) + EPS) * gain


def modulation_kernel(lat_hbm, ctx_hbm, scale_hbm, shift_hbm, gate_hbm, out_ref, cond_ref, act_ref, w_ref, sems):
    conds = [
        pltpu.make_async_copy(c, cond_ref.at[i], sems.at[3 + i]) for i, c in enumerate((lat_hbm, ctx_hbm))
    ]
    copies = [
        pltpu.make_async_copy(w, w_ref.at[i], sems.at[i])
        for i, w in enumerate((scale_hbm, shift_hbm, gate_hbm))
    ]
    for c in conds + copies:
        c.start()
    lines = w_ref.shape[1] // 128
    first = lax.axis_index("sp") * lines
    act = []
    for i, c in enumerate(conds):
        c.wait()
        v = cond_ref[i].astype(F32)
        act_ref[i] = v * jax.nn.sigmoid(v)
        act.append(jnp.concatenate([act_ref[i, pl.ds(first + j, 1), :] for j in range(lines)], axis=1))
    act = jnp.concatenate(act, axis=0).astype(BF16)
    pieces = w_ref.shape[2] // 128
    rows, context_rows = [], []
    for i, c in enumerate(copies):
        c.wait()
        part = jnp.dot(act, w_ref[i], preferred_element_type=F32)
        near = part[0:1].astype(BF16).astype(F32)
        rows += [near, part[0:1] - near]
        if i < 2:
            context_rows.append(part[1:2])
    tile = jnp.concatenate(
        [r[:, 128 * j:128 * j + 128] for r in rows + context_rows for j in range(pieces)], axis=0
    ).astype(BF16)
    for i in range(out_ref.shape[0]):
        out_ref[i] = tile


def sum_kernel(in_ref, out_ref):
    total = in_ref[0].astype(F32)
    for i in range(1, in_ref.shape[0]):
        total = total + in_ref[i].astype(F32)
    pieces = in_ref.shape[1] // 8
    for i in range(3):
        at = 2 * i * pieces
        out_ref[i * pieces:(i + 1) * pieces, :] = total[at:at + pieces] + total[at + pieces:at + 2 * pieces]
    out_ref[3 * pieces:5 * pieces, :] = total[6 * pieces:8 * pieces]
    out_ref[5 * pieces:, :] = jnp.zeros((out_ref.shape[0] - 5 * pieces, 128), F32)


def prepare_kernel(x_ref, c_ref, wk_ref, wv_ref, rx_ref, rc_ref, w_ref):
    tok, width = x_ref.shape
    step = 16

    def rows_of(src, dst, rows):
        total = jnp.zeros((step, 128), F32)
        for j in range(width // 128):
            v = src[rows, 128 * j:128 * j + 128].astype(F32)
            total = total + v * v
        r = lax.rsqrt(jnp.sum(total, axis=-1, keepdims=True) / width + EPS)
        dst[rows, :] = jnp.broadcast_to(r, (step, 128))

    @pl.loop(0, tok // step)
    def _(i):
        rows_of(x_ref, rx_ref, pl.ds(pl.multiple_of(i * step, step), step))

    for i in range(c_ref.shape[0] // step):
        rows_of(c_ref, rc_ref, pl.ds(i * step, step))

    @pl.loop(0, w_ref.shape[0] // 256)
    def _(i):
        rows = pl.ds(pl.multiple_of(i * 256, 256), 256)
        w_ref[rows, :HEAD] = wk_ref[rows, :]
        w_ref[rows, HEAD:] = wv_ref[rows, :]


def kv_kernel(
    x_ref, c_ref, rx_ref, rc_ref, own_ref, m1_ref, m3_ref, m2_ref, gain_ref, w_ref, g_ref, cos_ref, sin_ref,
    kv_ref, nm_ref, gate_ref, both_ref, mod_ref, ab_ref,
):
    tok, width = x_ref.shape
    ctx = c_ref.shape[0]
    n_tp = lax.axis_size("tp")
    chip, core = lax.axis_index("tp") // 2, lax.axis_index("tp") % 2
    n_x = n_tp // 2
    for back, ref in ((0, own_ref), (1, m1_ref), (3, m3_ref), (2, m2_ref)):
        source = lax.rem(chip + n_x - back, n_x)
        for c in range(2):
            mod_ref[2 * source + lax.rem(core + c, 2)] = ref[c]
    pieces = width // n_tp // 128
    for t in range(n_tp):
        for p in range(pieces):
            cs = slice((t * pieces + p) * 128, (t * pieces + p + 1) * 128)
            piece = [mod_ref[t, i * pieces + p:i * pieces + p + 1, :] for i in range(5)]
            gain = gain_ref[:, cs]
            ab_ref[0:1, cs] = gain * (1.0 + piece[0])
            ab_ref[1:2, cs] = piece[1]
            gate_ref[:, cs] = piece[2]
            ab_ref[2:3, cs] = gain * (1.0 + piece[3])
            ab_ref[3:4, cs] = piece[4]

    chunk, step = width // 4, 64
    both = None
    for k in range(0, width, chunk):
        for j in range(k, k + chunk, 128):
            cs = slice(j, j + 128)
            for i in range(0, tok, step):
                rows = slice(i, i + step)
                v = x_ref[rows, cs].astype(F32) * rx_ref[rows, :]
                nm_ref[rows, cs] = (v * ab_ref[0:1, cs] + ab_ref[1:2, cs]).astype(BF16)
            v = c_ref[:, cs].astype(F32) * rc_ref[...]
            nm_ref[tok:tok + ctx, cs] = (v * ab_ref[2:3, cs] + ab_ref[3:4, cs]).astype(BF16)
        part = jnp.dot(nm_ref[:, k:k + chunk], w_ref[k:k + chunk, :], preferred_element_type=F32)
        both = part if both is None else both + part
    both_ref[...] = both
    kv_ref[:, HEAD:] = both_ref[:, HEAD:].astype(BF16)
    gain = g_ref[...]
    tile = 128

    @pl.loop(0, tok // tile)
    def _(i):
        rows = pl.ds(pl.multiple_of(i * tile, tile), tile)
        k = rotate_rows(rms_head(both_ref[rows, :HEAD], gain), cos_ref[rows, :], sin_ref[rows, :])
        kv_ref[rows, :HEAD] = k.astype(BF16)

    kv_ref[tok:tok + ctx, :HEAD] = rms_head(both_ref[tok:tok + ctx, :HEAD], gain).astype(BF16)


def q_kernel(nm_ref, w_ref, g_ref, cos_ref, sin_ref, q_ref, both_ref):
    tok = cos_ref.shape[0]
    heads = w_ref.shape[1] // HEAD
    gain = g_ref[...]
    tile = 128
    both_ref[...] = jnp.dot(nm_ref[:tok, :], w_ref[...], preferred_element_type=F32)

    @pl.loop(0, tok // tile)
    def _(i):
        rows = pl.ds(pl.multiple_of(i * tile, tile), tile)
        for h in range(heads):
            v = rotate_rows(
                rms_head(both_ref[rows, h * HEAD:(h + 1) * HEAD], gain), cos_ref[rows, :], sin_ref[rows, :]
            )
            q_ref[pl.ds(pl.multiple_of(h * tok + i * tile, tile), tile), :] = v.astype(BF16)


def attend_block(q_ref, kv_refs, vt_refs, m_ref, l_ref, acc_ref, cols, latents):
    q = q_ref[cols, :]
    scores = []
    for kv_ref, lat in zip(kv_refs, latents, strict=True):
        s = lax.dot_general(kv_ref[:, :HEAD], q, (((1,), (1,)), ((), ())), preferred_element_type=F32)
        if lat < kv_ref.shape[0]:
            s = jnp.concatenate([s[:lat], s[lat:] + CONTEXT_LIFT / SCALING], axis=0)
        scores.append(s)
    old = m_ref[0:1, cols]
    new = old
    for s in scores:
        new = jnp.maximum(new, jnp.max(s, axis=0, keepdims=True))
    keep = jnp.exp2((old - new) * (SCALING * LOG2E))
    m_ref[0:1, cols] = new
    total = l_ref[0:1, cols] * keep
    out = acc_ref[:, cols] * keep
    for s, vt_ref in zip(scores, vt_refs, strict=True):
        p = jnp.exp2((s - new) * (SCALING * LOG2E))
        total = total + jnp.sum(p, axis=0, keepdims=True)
        out = out + jnp.dot(vt_ref[...], p.astype(BF16), preferred_element_type=F32)
    l_ref[0:1, cols] = total
    acc_ref[:, cols] = out


def attend_kernel(latents, first, last, tok, *refs):
    n_kv = len(latents)
    q_ref, kv_refs = refs[0], refs[1:1 + n_kv]
    at = 1 + n_kv
    if not first:
        m_in, l_in, acc_in = refs[at:at + 3]
        at += 3
    if last:
        out_ref = refs[at]
        at += 1
    m_ref, l_ref, acc_ref = refs[at:at + 3]
    vt_refs = refs[at + 3:]
    if first:
        m_ref[...] = jnp.full(m_ref.shape, -1e30, F32)
        l_ref[...] = jnp.zeros(l_ref.shape, F32)
        acc_ref[...] = jnp.zeros(acc_ref.shape, F32)
    else:
        m_ref[...] = m_in[...]
        l_ref[...] = l_in[...]
        acc_ref[...] = acc_in[...]
    for kv_ref, vt_ref in zip(kv_refs, vt_refs, strict=True):
        vt_ref[...] = jnp.transpose(kv_ref[:, HEAD:])
    queries = q_ref.shape[0]
    width = 256
    if last:
        attend_block(q_ref, kv_refs, vt_refs, m_ref, l_ref, acc_ref, slice(0, queries), latents)
        for h in range(queries // tok):
            cols = slice(h * tok, (h + 1) * tok)
            done = acc_ref[:, cols] / l_ref[0:1, cols]
            out_ref[:, h * HEAD:(h + 1) * HEAD] = jnp.transpose(done).astype(BF16)
    else:

        @pl.loop(0, queries // width)
        def _(i):
            cols = pl.ds(pl.multiple_of(i * width, width), width)
            attend_block(q_ref, kv_refs, vt_refs, m_ref, l_ref, acc_ref, cols, latents)


def attend(q, chunks, state, tok, last=False):
    queries = q.shape[0]
    first = state is None
    latents = [tok] * len(chunks)
    shapes = [
        jax.ShapeDtypeStruct((8, queries), F32),
        jax.ShapeDtypeStruct((8, queries), F32),
        jax.ShapeDtypeStruct((HEAD, queries), F32),
    ]
    rows = sum(c.shape[0] for c in chunks)
    turned = [pltpu.VMEM((HEAD, c.shape[0]), BF16) for c in chunks]
    cost = pl.CostEstimate(
        flops=4 * rows * queries * HEAD, transcendentals=rows * queries, bytes_accessed=1 << 20
    )
    operands = [q, *chunks] + ([] if first else list(state))
    kernel = functools.partial(attend_kernel, latents, first, last, tok)
    if last:
        return pl.pallas_call(
            kernel,
            out_shape=jax.ShapeDtypeStruct((tok, queries // tok * HEAD), BF16),
            in_specs=[VM] * len(operands),
            out_specs=VM,
            scratch_shapes=[*[pltpu.VMEM(s.shape, s.dtype) for s in shapes], *turned],
            cost_estimate=cost,
            compiler_params=pltpu.CompilerParams(vmem_limit_bytes=16 << 20),
            name="attend_last",
        )(*operands)
    return pl.pallas_call(
        kernel,
        out_shape=shapes,
        in_specs=[VM] * len(operands),
        out_specs=[VM] * 3,
        scratch_shapes=turned,
        input_output_aliases={} if first else {1 + len(chunks) + i: i for i in range(3)},
        cost_estimate=cost,
        compiler_params=pltpu.CompilerParams(vmem_limit_bytes=16 << 20),
        name="attend",
    )(*operands)


def shifted(x, axis, by):
    n = lax.axis_size(axis)
    return lax.ppermute(x, axis, [(i, (i + by) % n) for i in range(n)])


def along_ring(x, by):
    n_sp, n_tp = lax.axis_size("sp"), lax.axis_size("tp")
    pairs = []
    for z in range(n_sp):
        for t in range(n_tp):
            to = (z + (by if t % 2 else -by)) % n_sp
            pairs.append((z * n_tp + t, to * n_tp + t))
    return lax.ppermute(x, ("sp", "tp"), pairs)


def other_core(x):
    n = lax.axis_size("tp")
    return lax.ppermute(x, "tp", [(i, i ^ 1) for i in range(n)])


def body(
    latent, context, cond_latent, cond_context, w_shift, w_scale, w_gate, norm_gain,
    w_query, w_key, w_value, q_gain, k_gain, w_out,
):
    seq_index = lax.axis_index("sp")
    n_sp = lax.axis_size("sp")
    tp_index = lax.axis_index("tp")
    mod_rows, mod_cols = w_shift.shape
    tok, width = latent.shape
    ctx = context.shape[0]

    n_tp = lax.axis_size("tp")
    pieces = mod_cols // 128
    lines = -(-5 * pieces // 8) * 8
    partial_mod = pl.pallas_call(
        modulation_kernel,
        out_shape=jax.ShapeDtypeStruct((n_sp, 8 * pieces, 128), BF16),
        in_specs=[pl.BlockSpec(memory_space=pl.ANY)] * 5,
        out_specs=VM,
        scratch_shapes=[
            pltpu.VMEM((2, width // 128, 128), BF16),
            pltpu.VMEM((2, width // 128, 128), F32),
            pltpu.VMEM((3, mod_rows, mod_cols), BF16),
            pltpu.SemaphoreType.DMA((5,)),
        ],
        compiler_params=pltpu.CompilerParams(vmem_limit_bytes=60 << 20),
        name="modulation",
    )(cond_latent.reshape(-1, 128), cond_context.reshape(-1, 128), w_scale, w_shift, w_gate)
    gathered = lax.all_to_all(partial_mod, "sp", split_axis=0, concat_axis=0, tiled=True)
    rx, rc, w_kv = pl.pallas_call(
        prepare_kernel,
        out_shape=[
            jax.ShapeDtypeStruct((tok, 128), F32),
            jax.ShapeDtypeStruct((ctx, 128), F32),
            jax.ShapeDtypeStruct((width, 2 * HEAD), BF16),
        ],
        in_specs=[VM] * 4,
        out_specs=[VM] * 3,
        compiler_params=pltpu.CompilerParams(vmem_limit_bytes=32 << 20),
        cost_estimate=pl.CostEstimate(flops=1 << 30, transcendentals=0, bytes_accessed=12 << 20),
        name="prepare",
    )(latent, context, w_key, w_value)
    positions = seq_index * tok + jnp.arange(tok, dtype=jnp.int32)
    freqs = HEAD // 4
    inverse = ROPE_THETA ** (-jnp.arange(freqs, dtype=F32) / freqs)
    row = (positions // GRID_W).astype(F32)[:, None] * inverse
    col = (positions % GRID_W).astype(F32)[:, None] * inverse
    cos = jnp.concatenate([jnp.cos(row), jnp.cos(row), jnp.cos(col), jnp.cos(col)], axis=1)
    sin = jnp.concatenate([-jnp.sin(row), jnp.sin(row), -jnp.sin(col), jnp.sin(col)], axis=1)

    w_other = other_core(w_out)
    gathered, rx, rc, w_kv, cos, sin, w_other = lax.optimization_barrier((gathered, rx, rc, w_kv, cos, sin, w_other))
    summed = pl.pallas_call(
        sum_kernel,
        out_shape=jax.ShapeDtypeStruct((lines, 128), F32),
        in_specs=[VM],
        out_specs=VM,
        compiler_params=pltpu.CompilerParams(vmem_limit_bytes=8 << 20),
        cost_estimate=pl.CostEstimate(flops=8 << 30, transcendentals=0, bytes_accessed=1 << 20),
        name="sum_parts",
    )(gathered)
    pair = jnp.stack([summed, other_core(summed)])
    columns = [pair, shifted(pair, "tp", 2), shifted(pair, "tp", -2)]
    columns.append(shifted(pair, "tp", 4))

    kv, normed, gate = pl.pallas_call(
        kv_kernel,
        out_shape=[
            jax.ShapeDtypeStruct((tok + ctx, 2 * HEAD), BF16),
            jax.ShapeDtypeStruct((tok + ctx, width), BF16),
            jax.ShapeDtypeStruct((1, width), F32),
        ],
        in_specs=[VM] * 13,
        out_specs=[VM] * 3,
        scratch_shapes=[
            pltpu.VMEM((tok + ctx, 2 * HEAD), F32),
            pltpu.VMEM((n_tp, lines, 128), F32),
            pltpu.VMEM((8, width), F32),
        ],
        cost_estimate=pl.CostEstimate(flops=2 * tok * width * 256, transcendentals=0, bytes_accessed=1 << 22),
        compiler_params=pltpu.CompilerParams(vmem_limit_bytes=24 << 20),
        name="project_kv",
    )(
        latent, context, rx, rc, *columns, norm_gain.reshape(1, width), w_kv, k_gain.reshape(1, HEAD), cos, sin
    )

    right, left = along_ring(kv, 1), along_ring(kv, -1)
    q = pl.pallas_call(
        q_kernel,
        out_shape=jax.ShapeDtypeStruct((w_query.shape[1] // HEAD * tok, HEAD), BF16),
        in_specs=[VM] * 5,
        out_specs=VM,
        scratch_shapes=[pltpu.VMEM((tok, w_query.shape[1]), F32)],
        cost_estimate=pl.CostEstimate(flops=2 * tok * width * 256, transcendentals=0, bytes_accessed=1 << 22),
        compiler_params=pltpu.CompilerParams(vmem_limit_bytes=24 << 20),
        name="project_q",
    )(normed, w_query, q_gain.reshape(1, HEAD), cos, sin)
    state = attend(q, [kv], None, tok)
    half = n_sp // 2
    for step in range(1, half):
        right, m = lax.optimization_barrier((right, state[0]))
        now, right = right, along_ring(right, 1)
        state = attend(q, [now], [m, *state[1:]], tok)
        left, m = lax.optimization_barrier((left, state[0]))
        now = left
        if step + 1 < half:
            left = along_ring(left, -1)
        state = attend(q, [now], [m, *state[1:]], tok)
    attended = attend(q, [right], state, tok, last=True)

    n_x = lax.axis_size("tp") // 2
    core, chip = tp_index % 2, tp_index // 2
    share = tok // (2 * n_x)
    parts = attended.reshape(n_x, 2, share, attended.shape[1])
    parts = jnp.concatenate([parts, parts], axis=0)
    parts = lax.dynamic_slice_in_dim(parts, chip, n_x, 0)
    mine = lax.dynamic_index_in_dim(parts, core, 1, keepdims=False)
    theirs = lax.dynamic_index_in_dim(parts, 1 - core, 1, keepdims=False)
    far, near = (2,), (1, 3, 0)

    def product(side, weights, which):
        rows = jnp.concatenate([side[i] for i in which]) if len(which) > 1 else side[which[0]]
        return jnp.dot(rows, weights, preferred_element_type=F32)

    others = other_core(theirs)
    own_far, own_near = lax.optimization_barrier((product(mine, w_out, far), product(mine, w_out, near)))
    far_sum = (own_far + product(others, w_other, far)).astype(BF16)
    h = width // 2
    from_left = shifted(far_sum[:, :h], "tp", 2)
    from_right = shifted(far_sum[:, h:], "tp", -2)
    near_sum = own_near + product(others, w_other, near)
    nxt, prv, own = (near_sum[i * share:(i + 1) * share] for i in range(3))
    halves = (nxt[:, h:].astype(BF16), prv[:, :h].astype(BF16))
    a1 = shifted(halves[0], "tp", 2)
    b0 = shifted(halves[1], "tp", -2)
    joined = ((nxt[:, :h] + from_left.astype(F32)).astype(BF16), (prv[:, h:] + from_right.astype(F32)).astype(BF16))
    a0 = shifted(joined[0], "tp", 2)
    b1 = shifted(joined[1], "tp", -2)
    own, a0, a1, b0, b1 = lax.optimization_barrier((own, a0, a1, b0, b1))
    left_half = own[:, :h] + a0.astype(F32) + b0.astype(F32)
    right_half = own[:, h:] + a1.astype(F32) + b1.astype(F32)
    return (gate * jnp.concatenate([left_half, right_half], axis=1)).astype(BF16)


def solution(mesh):
    placed = (
        P(("grp", "sp"), None),
        P(("grp", "sp"), None),
        P("grp"),
        P(),
        P("sp", "tp"),
        P("sp", "tp"),
        P("sp", "tp"),
        P(),
        P(None, "tp"),
        P(None, "tp"),
        P(None, "tp"),
        P(),
        P(),
        P("tp", None),
    )
    return jax.shard_map(
        body, mesh=mesh, in_specs=placed, out_specs=P(("grp", "sp", "tp"), None), check_vma=False
    )
```
